32 devices in a mesh: ra: 8 (over z, y), cb: 4 (over x, core).
Axes of the slice: x: 2, y: 2, z: 4, core: 2. Of those that a mesh axis runs over, the one named last changes fastest.
Arguments:
- tokens: bfloat16 [2048, 4096], P('ra'), may hold values from -16 to 16
- norm_gain: float32 [2, 2048], replicated, may hold values from 0.1 to 1.9
- up_weight: float32 [2, 2048, 6144], P(None, 'ra', 'cb'), may hold values from -0.125 to 0.125
- gate_weight: float32 [2, 2048, 6144], P(None, 'ra', 'cb'), may hold values from -0.125 to 0.125
- up_scale: float32 [2, 6144], P(None, 'cb'), may hold values from 0.5 to 2
- gate_scale: float32 [2, 6144], P(None, 'cb'), may hold values from 0.5 to 2
- up_taps: float32 [2, 3, 6144], P(None, None, 'cb'), may hold values from -3 to 3
- gate_taps: float32 [2, 3, 6144], P(None, None, 'cb'), may hold values from -3 to 3
- down_weight: float32 [2, 2048, 6144], P(None, 'ra', 'cb'), may hold values from -0.078125 to 0.078125
- down_scale: float32 [2, 2048], replicated, may hold values from 0.5 to 2
Outputs:
- mixed: bfloat16 [2048, 4096], P('ra')
The draws below stay inside these ranges and needn't reach their ends.
All inputs are finite; a program needn't handle non-finite values.
Results may differ from the reference program's by a relative error of at most 0.024.
Values may be sent and summed in bfloat16 or wider, within the bound.
A program may use at most 128 MiB of HBM per device.

```python
import math
import jax
import jax.numpy as jnp
from jax import lax

D = 2048
FF = 6144
KW = 3
LAYERS = 2
TOKENS = 4096
N_RA = 8
N_CB = 4


def draw_tokens(key, part):
    first, second, third = jax.random.split(key, 3)
    blocks = jnp.exp(jax.random.uniform(second, (N_RA,), jnp.float32, math.log(0.3), math.log(3.0)))
    features = jnp.repeat(blocks, D // N_RA, total_repeat_length=D)
    base = jnp.clip(jax.random.normal(first, (D, TOKENS), jnp.float32), -4.0, 4.0)
    return (base * features[:, None]).astype(jnp.bfloat16)


def shard_levels(rng, extent, cuts, smallest, high):
    gain, own = 1.0, jax.random.fold_in(rng, 6)
    for position, parts in cuts:
        draws = jnp.exp(jax.random.uniform(jax.random.fold_in(own, position), (parts,), jnp.float32, smallest / len(cuts), high / len(cuts)))
        gain = gain * jnp.repeat(draws, extent[position] // parts).reshape([-1 if axis == position else 1 for axis in range(len(extent))])
    return gain


def normal_values(stream_key, extent, scale, bound, pieces=(), dtype=jnp.bfloat16):
    level = shard_levels(stream_key, extent, pieces, -0.22, 0.18) if pieces else 1.0
    values = jax.random.normal(stream_key, extent, jnp.float32) * scale * level
    return jnp.minimum(jnp.maximum(values, -bound), bound).astype(dtype)


def setup_inputs(seed: int = 0) -> dict:
    splits = jax.random.split(jax.random.key(seed), 11)
    return {
        "tokens": draw_tokens(jax.random.fold_in(splits[10], 71), 0),
        "norm_gain": jnp.clip(1.0 + 0.18 * jax.random.normal(splits[1], (LAYERS, D), jnp.float32), 0.1, 1.9),
        "up_weight": normal_values(splits[2], (LAYERS, D, FF), D ** -0.5, 0.125, ((1, 8), (2, 4)), jnp.float32),
        "gate_weight": normal_values(splits[3], (LAYERS, D, FF), D ** -0.5, 0.125, ((1, 8), (2, 4)), jnp.float32),
        "up_scale": jnp.clip(jnp.exp(math.log(2.0) - 1.3862944 * jax.random.uniform(splits[4], (LAYERS, FF), jnp.float32) ** shard_levels(splits[4], (LAYERS, FF), ((1, 4),), -0.2, 0.2)), 0.5, 2.0),
        "gate_scale": jnp.clip(jnp.exp(math.log(2.0) - 1.3862944 * jax.random.uniform(splits[5], (LAYERS, FF), jnp.float32) ** shard_levels(splits[5], (LAYERS, FF), ((1, 4),), -0.2, 0.2)), 0.5, 2.0),
        "up_taps": normal_values(splits[6], (LAYERS, KW, FF), 0.6, 3.0, ((2, 4),), jnp.float32),
        "gate_taps": normal_values(splits[7], (LAYERS, KW, FF), 0.6, 3.0, ((2, 4),), jnp.float32),
        "down_weight": normal_values(splits[8], (LAYERS, D, FF), FF ** -0.5, 0.078125, ((1, 8), (2, 4)), jnp.float32),
        "down_scale": jnp.clip(jnp.exp(jax.random.uniform(splits[9], (LAYERS, D), jnp.float32, math.log(0.5), math.log(2.0))), 0.5, 2.0),
    }


EPS = 1e-06
RESIDUAL = 0.5

def causal_taps(values, taps):
    width = taps.shape[0]
    length = values.shape[0]
    padded = jnp.pad(values, ((width - 1, 0), (0, 0)))
    total = jnp.zeros_like(values)
    for k in range(width):
        total = total + taps[k][None, :] * padded[k:k + length]
    return total

def reference(tokens, norm_gain, up_weight, gate_weight, up_scale, gate_scale, up_taps, gate_taps, down_weight, down_scale):
    state = tokens.T
    block = FF // N_CB
    for layer in range(LAYERS):
        state_f = state.astype(jnp.float32)
        inverse = lax.rsqrt(lax.optimization_barrier(jnp.mean(state_f * state_f, axis=1, keepdims=True)) + EPS)
        scaled = (state_f * norm_gain[layer][None, :]).astype(jnp.bfloat16)
        up_raw = jnp.dot(scaled, up_weight[layer].astype(jnp.bfloat16), preferred_element_type=jnp.float32)
        gate_raw = jnp.dot(scaled, gate_weight[layer].astype(jnp.bfloat16), preferred_element_type=jnp.float32)
        up_pre = up_raw * inverse * up_scale[layer][None, :]
        gate_pre = gate_raw * inverse * gate_scale[layer][None, :]
        conv_up = causal_taps(up_pre, up_taps[layer])
        conv_gate = causal_taps(gate_pre, gate_taps[layer])
        hidden = (jax.nn.silu(conv_gate) * conv_up).astype(jnp.bfloat16)
        weight_b = down_weight[layer].astype(jnp.bfloat16)
        down = jnp.zeros((hidden.shape[0], weight_b.shape[0]), jnp.float32)
        for group in range(N_CB):
            term = jnp.dot(hidden[:, group * block:(group + 1) * block], weight_b[:, group * block:(group + 1) * block].T, preferred_element_type=jnp.float32)
            rounded = lax.optimization_barrier(term.astype(jnp.bfloat16))
            down = down + rounded.astype(jnp.float32)
        state = (down * down_scale[layer][None, :] + RESIDUAL * state_f).astype(jnp.bfloat16)
    return state.T
```

```python
import functools

import jax
import jax.numpy as jnp
from jax import lax
from jax.experimental import pallas as pl
from jax.experimental.pallas import tpu as pltpu
from jax.sharding import PartitionSpec as P

EPS = 1e-06
RESIDUAL = 0.5
MESH = pl.DeviceIdType.MESH


def doublings(low, high):
    bits = []
    while low < high:
        bits.append(low)
        low *= 2
    return bits


def bit_of(value, bit):
    return lax.rem(lax.div(value, bit), 2) if not isinstance(value, int) else (value // bit) % 2


def flip(value, offset):
    for bit in doublings(1, offset + 1):
        if offset & bit:
            value = value + bit - 2 * bit * bit_of(value, bit)
    return value


class Plan:
    def __init__(self, n_ra, n_cb, rows, columns, length, layers, width):
        self.n_ra, self.n_cb, self.rows, self.columns = n_ra, n_cb, rows, columns
        self.length, self.layers, self.width = length, layers, width
        self.n_y = 1 << ((n_ra.bit_length() - 1) // 2)
        self.n_z = n_ra // self.n_y
        self.half = columns // 2
        self.groups = n_ra // 2
        self.group_tokens = length // self.groups
        self.cb_bits = doublings(1, n_cb)
        self.n_steps = len(self.cb_bits) + 1
        self.sizes = [self.group_tokens >> (s + 1) for s in range(self.n_steps)]
        self.own = self.sizes[-1]
        self.q = 1
        while rows * self.q < 256 and self.q < self.n_y:
            self.q *= 2
        self.chunk = rows * self.q
        self.n_chunks = n_ra // self.q
        self.features = n_ra * rows
        cy = self.n_y // self.q
        self.cy = cy
        self.order_bits = [cy] + doublings(2 * cy, self.n_z * cy) + doublings(1, cy)
        self.edge = 8


def kernel(
    p,
    tin,
    up_w,
    gate_w,
    down_w,
    gain,
    up_scale,
    gate_scale,
    up_taps,
    gate_taps,
    down_scale,
    out,
    w,
    give,
    stage,
    st,
    up,
    gate,
    hid,
    tok,
    sq,
    halo,
    obuf,
    ost,
    accs,
    snds,
    rcvs,
    sem,
):
    r, j = lax.axis_index("ra"), lax.axis_index("cb")
    z, y = lax.div(r, p.n_y), lax.rem(r, p.n_y)
    m = lax.rem(z, 2)
    mine = [bit_of(j, bit) for bit in p.cb_bits] + [m]
    n_k = 3 * p.layers

    def group_of(dev):
        return lax.div(lax.div(dev, p.n_y), 2) * p.n_y + lax.rem(dev, p.n_y)

    def sub_row(bits, count):
        start = 0
        for s in range(count):
            start = start + bits[s] * p.sizes[s]
        return start

    def first_token(dev):
        bits = mine[:-1] + [lax.rem(lax.div(dev, p.n_y), 2)]
        return group_of(dev) * p.group_tokens + sub_row(bits, p.n_steps)

    def partner(s):
        if s < p.n_steps - 1:
            return r, flip(j, p.cb_bits[s])
        return flip(r, p.n_y), j

    def copy(src, dst, ssem, rsem, dev):
        return pltpu.make_async_remote_copy(
            src_ref=src,
            dst_ref=dst,
            send_sem=ssem,
            recv_sem=rsem,
            device_id=dev,
            device_id_type=MESH,
        )

    def at_rows(start, size):
        return pl.ds(pl.multiple_of(start, size), size)

    own_row = sub_row(mine, p.n_steps)
    own_rows = at_rows(own_row, p.own)
    my_slab = at_rows(r * p.rows, p.rows)

    barrier = pltpu.get_barrier_semaphore()
    for off in range(1, p.n_ra):
        pl.semaphore_signal(barrier, inc=1, device_id=(flip(r, off), j), device_id_type=MESH)
    for bit in p.cb_bits:
        pl.semaphore_signal(barrier, inc=1, device_id=(r, flip(j, bit)), device_id_type=MESH)

    def load(k):
        layer, kind = k // 3, k % 3
        source = (up_w, gate_w, down_w)[kind]
        return pltpu.make_async_copy(source.at[layer], stage.at[k % 2], sem["stage"].at[k % 2])

    load(0).start()
    load(1).start()
    own_tokens = pltpu.make_async_copy(
        tin.at[at_rows(first_token(r), p.own)], tok.at[r], sem["local"].at[0]
    )
    own_tokens.start()
    pl.semaphore_wait(barrier, p.n_ra - 1 + len(p.cb_bits))

    def token_send(off):
        dev = flip(r, off)
        return copy(
            tin.at[at_rows(first_token(dev), p.own)],
            tok.at[r],
            sem["tok_s"].at[off],
            sem["tok_r"].at[r],
            (dev, j),
        )

    for off in range(1, p.n_ra):
        token_send(off).start()

    def slab(k, dev):
        return w.at[k, at_rows(dev * p.rows, p.rows)]

    def z_send(k, dz):
        source = give.at[k] if dz % 2 else slab(k, r)
        return copy(
            source, slab(k, r), sem["z"].at[k, dz], sem["w"].at[k, r], (flip(z, dz) * p.n_y + y, j)
        )

    def y_send(k, dz, dy):
        dev = flip(z, dz) * p.n_y + y
        return copy(
            slab(k, dev),
            slab(k, dev),
            sem["y"].at[k, dz, dy],
            sem["w"].at[k, dev],
            (z * p.n_y + flip(y, dy), j),
        )

    def slab_wait(k, dev):
        copy(slab(k, dev), slab(k, dev), sem["z"].at[k, 0], sem["w"].at[k, dev], (r, j)).wait_recv()

    def forward(k, dz):
        if dz:
            slab_wait(k, flip(z, dz) * p.n_y + y)
        for dy in range(1, p.n_y):
            y_send(k, dz, dy).start()

    def convert(k):
        load(k).wait()
        tile = min(64, p.rows)

        @pl.loop(0, p.rows // tile)
        def _(t):
            rows = at_rows(t * tile, tile)
            keep = stage[k % 2, rows, pl.ds(pl.multiple_of(m * p.half, 128), p.half)]
            rest = stage[k % 2, rows, pl.ds(pl.multiple_of((1 - m) * p.half, 128), p.half)]
            w[k, at_rows(r * p.rows + t * tile, tile), :] = keep.astype(jnp.bfloat16)
            give[k, rows, :] = rest.astype(jnp.bfloat16)

        if k + 2 < n_k:
            load(k + 2).start()

    far = list(range(2, p.n_z))

    def first_sends(k):
        z_send(k, 1).start()
        if k < 2:
            for dy in range(1, p.n_y):
                y_send(k, 0, dy).start()
        if 1 <= k <= 3:
            for dz in far:
                z_send(k - 1, dz).start()

    convert(0)

    own_tokens.wait()
    for src in range(p.n_ra):
        lanes = slice(src * p.rows, (src + 1) * p.rows)

        @pl.when(r != src)
        def _():
            copy(
                tok.at[src], tok.at[src], sem["tok_s"].at[0], sem["tok_r"].at[src], (r, j)
            ).wait_recv()

        st[0, own_rows, lanes] = tok[src]

    def block_rows(a):
        count = p.n_steps - a
        size = p.own << a
        return sub_row(mine, count), size

    def gather_copy(layer, a, lanes, ssem, rsem):
        start, size = block_rows(a)
        ref = st.at[layer, at_rows(start, size), lanes]
        return copy(ref, ref, ssem, rsem, partner(p.n_steps - 1 - a))

    def gather_wait(layer, a, lanes, ssem, rsem):
        start, size = block_rows(a)
        s = p.n_steps - 1 - a
        ref = st.at[layer, at_rows(start + (1 - 2 * mine[s]) * size, size), lanes]
        copy(ref, ref, ssem, rsem, (r, j)).wait_recv()

    everything = pl.ds(0, p.features)

    def gather0(a):
        return gather_copy(0, a, everything, sem["g0_s"].at[a], sem["g0_r"].at[a])

    def gather0_wait(a):
        gather_wait(0, a, everything, sem["g0_s"].at[a], sem["g0_r"].at[a])

    convert(1)
    gather0(0).start()
    for k in range(2, n_k):
        first_sends(k - 2)
        convert(k)
    first_sends(n_k - 2)
    first_sends(n_k - 1)

    for a in range(p.n_steps):
        gather0_wait(a)
        if a + 1 < p.n_steps:
            gather0(a + 1).start()
        if a < 2:
            forward(a, 1)

    def chunk_of(i):
        base = (z - m) * p.cy + lax.div(y, p.q)
        total = 0
        shift = 1
        for bit in p.order_bits:
            total = total + lax.rem(lax.div(base, bit) + lax.div(i, shift), 2) * bit
            shift *= 2
        return total

    def chunk_lanes(f):
        return pl.ds(pl.multiple_of(f * p.chunk, p.chunk), p.chunk)

    def chunk_wait(k, f):
        for t in range(p.q):
            dev = f * p.q + t

            @pl.when(lax.rem(dev, p.n_y) != y)
            def _():
                slab_wait(k, dev)

    tile = min(256, p.group_tokens)
    fine = 64

    def squares(layer, lanes, first):
        @pl.loop(0, p.group_tokens // fine)
        def _(t):
            rows = at_rows(t * fine, fine)
            values = st[layer, rows, lanes].astype(jnp.float32)
            total = None
            for c in range(p.chunk // 128):
                part = values[:, c * 128 : (c + 1) * 128]
                total = part * part if total is None else total + part * part
            if first is None:
                sq[rows, :] = sq[rows, :] + total
            else:

                @pl.when(first)
                def _():
                    sq[rows, :] = total

                @pl.when(jnp.logical_not(first))
                def _():
                    sq[rows, :] = sq[rows, :] + total

    @pl.loop(0, p.n_chunks)
    def _(i):
        squares(0, chunk_lanes(i), i == 0)

    def product(layer, k, dst):
        @pl.loop(0, p.n_chunks)
        def _(i):
            f = chunk_of(i)
            chunk_wait(k, f)
            lanes = chunk_lanes(f)
            weights = w.at[k, at_rows(f * p.chunk, p.chunk)]

            @pl.loop(0, p.group_tokens // tile)
            def _(t):
                rows = at_rows(t * tile, tile)
                scaled = st[layer, rows, lanes].astype(jnp.float32) * gain[layer : layer + 1, lanes]
                term = jnp.dot(
                    scaled.astype(jnp.bfloat16), weights[...], preferred_element_type=jnp.float32
                )
                to = pl.ds(pl.multiple_of(p.edge + t * tile, 8), tile)

                @pl.when(i == 0)
                def _():
                    dst[to, :] = term

                @pl.when(i > 0)
                def _():
                    dst[to, :] = dst[to, :] + term

    own_half = pl.ds(pl.multiple_of(m * p.half, 128), p.half)
    group = group_of(r)
    following = group + 1
    following_dev = (lax.div(following, p.n_y) * 2 + m) * p.n_y + lax.rem(following, p.n_y)

    def halo_copy(layer, which):
        source = (up, gate)[which]
        return copy(
            source.at[pl.ds(p.group_tokens, p.edge)],
            halo.at[layer, which],
            sem["h_s"].at[layer, which],
            sem["h_r"].at[layer, which],
            (following_dev, j),
        )

    def convolve(layer):
        scale_u = up_scale[layer : layer + 1, own_half]
        scale_g = gate_scale[layer : layer + 1, own_half]

        @pl.loop(0, p.group_tokens // fine)
        def _(t):
            total = jnp.sum(sq[at_rows(t * fine, fine), :], axis=1, keepdims=True)
            inverse = lax.rsqrt(total * (1.0 / p.features) + EPS)
            rows = pl.ds(pl.multiple_of(p.edge + t * fine, 8), fine)
            up[rows, :] = up[rows, :] * inverse * scale_u
            gate[rows, :] = gate[rows, :] * inverse * scale_g

        @pl.when(following < p.groups)
        def _():
            halo_copy(layer, 0).start()
            halo_copy(layer, 1).start()

        @pl.when(group > 0)
        def _():
            for which, dst in ((0, up), (1, gate)):
                copy(
                    halo.at[layer, which],
                    halo.at[layer, which],
                    sem["h_s"].at[layer, which],
                    sem["h_r"].at[layer, which],
                    (r, j),
                ).wait_recv()
                dst[0 : p.edge, :] = halo[layer, which]

        @pl.when(group == 0)
        def _():
            up[0 : p.edge, :] = jnp.zeros((p.edge, p.half), jnp.float32)
            gate[0 : p.edge, :] = jnp.zeros((p.edge, p.half), jnp.float32)

        taps_u = up_taps[layer, :, own_half]
        taps_g = gate_taps[layer, :, own_half]

        def taps_over(ref, taps, t):
            values = ref[pl.ds(pl.multiple_of(t * fine, 8), fine + p.edge), :]
            low = p.edge + 1 - p.width
            total = taps[0:1] * values[low : low + fine]
            for c in range(1, p.width):
                total = total + taps[c : c + 1] * values[low + c : low + c + fine]
            return total

        @pl.loop(0, p.group_tokens // fine)
        def _(t):
            conv_gate = taps_over(gate, taps_g, t)
            conv_up = taps_over(up, taps_u, t)
            value = conv_gate / (1.0 + jnp.exp(-conv_gate)) * conv_up
            hid[at_rows(t * fine, fine), :] = value.astype(jnp.bfloat16)

    def reduce_copy(layer, s, i):
        return copy(
            snds[s].at[i],
            rcvs[s].at[layer, i],
            sem["r_s"].at[layer, s, i],
            sem["r_r"].at[layer, s, i],
            partner(s),
        )

    def reduce_wait(layer, s, i):
        ref = rcvs[s].at[layer, i]
        copy(ref, ref, sem["r_s"].at[layer, s, i], sem["r_r"].at[layer, s, i], (r, j)).wait_recv()

    def down_stage(layer, i):
        k = 3 * layer + 2
        f = chunk_of(i)
        chunk_wait(k, f)
        weights = w.at[k, at_rows(f * p.chunk, p.chunk)]
        size = p.sizes[0]
        step = min(tile, size)

        def term(start):
            return lax.dot_general(
                hid[pl.ds(pl.multiple_of(start, step), step), :],
                weights[...],
                (((1,), (1,)), ((), ())),
                preferred_element_type=jnp.float32,
            )

        @pl.loop(0, size // step)
        def _(t):
            rows = at_rows(t * step, step)
            snds[0][i, rows, :] = term((1 - mine[0]) * size + t * step).astype(jnp.bfloat16)

        @pl.loop(0, size // step)
        def _(t):
            accs[0][at_rows(t * step, step), :] = term(mine[0] * size + t * step)

        reduce_copy(layer, 0, i).start()

    def reduce_stage(layer, s, i):
        reduce_wait(layer, s - 1, i)
        size = p.sizes[s]
        give_rows = at_rows((1 - mine[s]) * size, size)
        keep_rows = at_rows(mine[s] * size, size)
        arrived = rcvs[s - 1][layer, i, give_rows, :].astype(jnp.float32)
        snds[s][i] = (accs[s - 1][give_rows, :] + arrived).astype(jnp.bfloat16)
        arrived = rcvs[s - 1][layer, i, keep_rows, :].astype(jnp.float32)
        accs[s][...] = accs[s - 1][keep_rows, :] + arrived
        reduce_copy(layer, s, i).start()

    def gather1(a, f):
        return gather_copy(1, a, chunk_lanes(f), sem["g_s"].at[a, f], sem["g_r"].at[a, f])

    def gather1_wait(a, f):
        gather_wait(1, a, chunk_lanes(f), sem["g_s"].at[a, f], sem["g_r"].at[a, f])

    def out_copy(f, t):
        return copy(
            ost.at[f, t],
            obuf.at[at_rows(first_token(r), p.own)],
            sem["o_s"].at[f, t],
            sem["o_r"].at[r],
            (f * p.q + t, j),
        )

    def last_stage(layer, i):
        f = chunk_of(i)
        s = p.n_steps - 1
        reduce_wait(layer, s, i)
        lanes = chunk_lanes(f)
        total = accs[s][...] + rcvs[s][layer, i].astype(jnp.float32)
        before = st[layer, own_rows, lanes].astype(jnp.float32)
        value = total * down_scale[layer : layer + 1, lanes] + RESIDUAL * before
        value = value.astype(jnp.bfloat16)
        if layer + 1 < p.layers:
            st[layer + 1, own_rows, lanes] = value
            gather1(0, f).start()
        else:
            for t in range(p.q):
                ost[f, t] = value[:, t * p.rows : (t + 1) * p.rows]
                dev = f * p.q + t

                @pl.when(dev == r)
                def _():
                    obuf[at_rows(first_token(r), p.own), :] = ost[f, t]

                @pl.when(dev != r)
                def _():
                    out_copy(f, t).start()

    def gather_stage(a, i):
        f = chunk_of(i)
        gather1_wait(a, f)
        if a + 1 < p.n_steps:
            gather1(a + 1, f).start()
        else:
            squares(1, chunk_lanes(f), i == 0)

    def pipeline(stages, tasks):
        count = p.n_chunks + len(stages) - 1

        @pl.loop(0, count)
        def _(it):
            for back in reversed(range(len(stages))):
                i = it - back

                @pl.when(jnp.logical_and(i >= 0, i < p.n_chunks))
                def _():
                    stages[back](i)

            for index, task in enumerate(tasks):

                @pl.when(it == 1 + index * (count - 2) // len(tasks))
                def _():
                    task()

    def pump(k):
        for dz in far:
            forward(k, dz)
        if k + 2 < n_k:
            forward(k + 2, 0)
            forward(k + 2, 1)

    for layer in range(p.layers):
        last = layer + 1 == p.layers
        k = 3 * layer
        if layer:
            for dz in far:
                z_send(k + 2, dz).start()
        pump(k)
        product(layer, k, up)
        pump(k + 1)
        product(layer, k + 1, gate)
        convolve(layer)
        pump(k + 2)
        stages = [functools.partial(down_stage, layer)]
        stages += [functools.partial(reduce_stage, layer, s) for s in range(1, p.n_steps)]
        stages += [functools.partial(last_stage, layer)]
        tasks = []
        if not last:
            stages += [functools.partial(gather_stage, a) for a in range(p.n_steps)]
            tasks = [
                lambda k=k, dz=dz: z_send(k, dz).start() for k in (k + 3, k + 4) for dz in far
            ]
        pipeline(stages, tasks)

        @pl.loop(0, p.n_chunks)
        def _(i):
            for s in range(p.n_steps):
                reduce_copy(layer, s, i).wait_send()

        @pl.when(following < p.groups)
        def _():
            halo_copy(layer, 0).wait_send()
            halo_copy(layer, 1).wait_send()

    sources = [
        (pz, py)
        for py in range(p.n_y)
        for pz in range(0, p.n_z, 2)
    ]
    n_out = p.n_steps - 1

    def out_rows(index, a, flipped):
        pz, py = sources[index]
        dev = flip(z, pz) * p.n_y + flip(y, py)
        start, size = block_rows(a)
        if flipped:
            start = start + (1 - 2 * mine[p.n_steps - 1 - a]) * size
        return obuf.at[at_rows(group_of(dev) * p.group_tokens + start, size)]

    def out_gather(index, a):
        ref = out_rows(index, a, False)
        return copy(
            ref,
            ref,
            sem["oa_s"].at[a - 1, index],
            sem["oa_r"].at[a - 1, index],
            partner(p.n_steps - 1 - a),
        )

    for index, (pz, py) in enumerate(sources):
        for low in range(2):
            dev = flip(z - m + low, pz) * p.n_y + flip(y, py)

            @pl.when(dev != r)
            def _():
                ref = obuf.at[at_rows(first_token(dev), p.own)]
                copy(ref, ref, sem["o_s"].at[0, 0], sem["o_r"].at[dev], (r, j)).wait_recv()

        out_gather(index, 1).start()
    for a in range(1, p.n_steps):
        for index in range(len(sources)):
            ref = out_rows(index, a, True)
            copy(
                ref, ref, sem["oa_s"].at[a - 1, index], sem["oa_r"].at[a - 1, index], (r, j)
            ).wait_recv()
            if a + 1 < p.n_steps:
                out_gather(index, a + 1).start()

    result = pltpu.make_async_copy(obuf, out, sem["local"].at[0])
    result.start()
    for off in range(1, p.n_ra):
        token_send(off).wait_send()
    for k in range(n_k):
        for dz in range(1, p.n_z):
            z_send(k, dz).wait_send()
        for dz in range(p.n_z):
            for dy in range(1, p.n_y):
                y_send(k, dz, dy).wait_send()
    for a in range(p.n_steps):
        gather0(a).wait_send()

    @pl.loop(0, p.n_chunks)
    def _(f):
        for a in range(p.n_steps):
            gather1(a, f).wait_send()
        for t in range(p.q):

            @pl.when(f * p.q + t != r)
            def _():
                out_copy(f, t).wait_send()

    for a in range(1, p.n_steps):
        for index in range(len(sources)):
            out_gather(index, a).wait_send()
    result.wait()


def per_device(
    tokens,
    norm_gain,
    up_weight,
    gate_weight,
    up_scale,
    gate_scale,
    up_taps,
    gate_taps,
    down_weight,
    down_scale,
):
    layers, rows, columns = up_weight.shape
    p = Plan(
        lax.axis_size("ra"),
        lax.axis_size("cb"),
        rows,
        columns,
        tokens.shape[1],
        layers,
        up_taps.shape[1],
    )
    n_k = 3 * layers
    bf16, f32 = jnp.bfloat16, jnp.float32
    dma = pltpu.SemaphoreType.DMA
    in_hbm = pl.BlockSpec(memory_space=pl.ANY)
    in_vmem = pl.BlockSpec(memory_space=pltpu.VMEM)
    sems = {
        "stage": dma((2,)),
        "local": dma((1,)),
        "tok_s": dma((p.n_ra,)),
        "tok_r": dma((p.n_ra,)),
        "w": dma((n_k, p.n_ra)),
        "z": dma((n_k, p.n_z)),
        "y": dma((n_k, p.n_z, p.n_y)),
        "g0_s": dma((p.n_steps,)),
        "g0_r": dma((p.n_steps,)),
        "g_s": dma((p.n_steps, p.n_chunks)),
        "g_r": dma((p.n_steps, p.n_chunks)),
        "r_s": dma((layers, p.n_steps, p.n_chunks)),
        "r_r": dma((layers, p.n_steps, p.n_chunks)),
        "h_s": dma((layers, 2)),
        "h_r": dma((layers, 2)),
        "o_s": dma((p.n_chunks, p.q)),
        "o_r": dma((p.n_ra,)),
        "oa_s": dma((p.n_steps - 1, p.groups)),
        "oa_r": dma((p.n_steps - 1, p.groups)),
    }
    names = list(sems)
    n_s = p.n_steps

    def body(*refs):
        head, rest = refs[:11 + 12], refs[11 + 12 :]
        accs, snds, rcvs = rest[:n_s], rest[n_s : 2 * n_s], rest[2 * n_s : 3 * n_s]
        kernel(p, *head, accs, snds, rcvs, dict(zip(names, rest[3 * n_s :])))

    turned = pl.pallas_call(
        body,
        out_shape=jax.ShapeDtypeStruct((p.length, rows), bf16),
        in_specs=[in_hbm] * 4 + [in_vmem] * 6,
        out_specs=in_hbm,
        scratch_shapes=[
            pltpu.VMEM((n_k, p.features, p.half), bf16),
            pltpu.VMEM((n_k, rows, p.half), bf16),
            pltpu.VMEM((2, rows, columns), f32),
            pltpu.VMEM((layers, p.group_tokens, p.features), bf16),
            pltpu.VMEM((p.edge + p.group_tokens, p.half), f32),
            pltpu.VMEM((p.edge + p.group_tokens, p.half), f32),
            pltpu.VMEM((p.group_tokens, p.half), bf16),
            pltpu.VMEM((p.n_ra, p.own, rows), bf16),
            pltpu.VMEM((p.group_tokens, 128), f32),
            pltpu.VMEM((layers, 2, p.edge, p.half), f32),
            pltpu.VMEM((p.length, rows), bf16),
            pltpu.VMEM((p.n_chunks, p.q, p.own, rows), bf16),
        ]
        + [pltpu.VMEM((size, p.chunk), f32) for size in p.sizes]
        + [pltpu.VMEM((p.n_chunks, size, p.chunk), bf16) for size in p.sizes]
        + [pltpu.VMEM((layers, p.n_chunks, size, p.chunk), bf16) for size in p.sizes]
        + [sems[name] for name in names],
        compiler_params=pltpu.CompilerParams(
            collective_id=0, has_side_effects=True, vmem_limit_bytes=66 * 1000 * 1000
        ),
        name="layers",
    )(
        tokens.T,
        up_weight,
        gate_weight,
        down_weight,
        norm_gain,
        up_scale,
        gate_scale,
        up_taps,
        gate_taps,
        down_scale,
    )
    return turned.T


def solution(mesh):
    placed = (
        P("ra", None),
        P(),
        P(None, "ra", "cb"),
        P(None, "ra", "cb"),
        P(None, "cb"),
        P(None, "cb"),
        P(None, None, "cb"),
        P(None, None, "cb"),
        P(None, "ra", "cb"),
        P(),
    )
    return jax.shard_map(
        per_device, mesh=mesh, in_specs=placed, out_specs=P("ra", None), check_vma=False
    )
```

```python
import functools

import jax
import jax.numpy as jnp
from jax import lax
from jax.experimental import pallas as pl
from jax.experimental.pallas import tpu as pltpu
from jax.sharding import PartitionSpec as P

EPS = 1e-06
RESIDUAL = 0.5
MESH = pl.DeviceIdType.MESH


def doublings(low, high):
    bits = []
    while low < high:
        bits.append(low)
        low *= 2
    return bits


def bit_of(value, bit):
    return lax.rem(lax.div(value, bit), 2) if not isinstance(value, int) else (value // bit) % 2


def flip(value, offset):
    for bit in doublings(1, offset + 1):
        if offset & bit:
            value = value + bit - 2 * bit * bit_of(value, bit)
    return value


class Plan:
    def __init__(self, n_ra, n_cb, rows, columns, length, layers, width):
        self.n_ra, self.n_cb, self.rows, self.columns = n_ra, n_cb, rows, columns
        self.length, self.layers, self.width = length, layers, width
        self.n_y = 1 << ((n_ra.bit_length() - 1) // 2)
        self.n_z = n_ra // self.n_y
        self.half = columns // 2
        self.groups = n_ra // 2
        self.group_tokens = length // self.groups
        self.cb_bits = doublings(1, n_cb)
        self.n_steps = len(self.cb_bits) + 1
        self.sizes = [self.group_tokens >> (s + 1) for s in range(self.n_steps)]
        self.own = self.sizes[-1]
        self.q = 1
        while rows * self.q < 256 and self.q < self.n_y:
            self.q *= 2
        self.chunk = rows * self.q
        self.n_chunks = n_ra // self.q
        self.features = n_ra * rows
        cy = self.n_y // self.q
        self.cy = cy
        self.order_bits = [cy] + doublings(1, cy) + doublings(2 * cy, self.n_z * cy)
        self.edge = 8
        self.extra = 16
        self.slots = 3


def kernel(
    p,
    tin,
    up_w,
    gate_w,
    down_w,
    gain,
    up_scale,
    gate_scale,
    up_taps,
    gate_taps,
    down_scale,
    out,
    w,
    give,
    stage,
    st,
    up,
    gate,
    hid,
    tok,
    tok_e,
    st_e,
    up_e,
    gate_e,
    sq_e,
    sq,
    halo,
    obuf,
    ost,
    accs,
    snds,
    rcvs,
    sem,
):
    r, j = lax.axis_index("ra"), lax.axis_index("cb")
    z, y = lax.div(r, p.n_y), lax.rem(r, p.n_y)
    m = lax.rem(z, 2)
    mine = [bit_of(j, bit) for bit in p.cb_bits] + [m]
    n_k = 3 * p.layers

    def group_of(dev):
        return lax.div(lax.div(dev, p.n_y), 2) * p.n_y + lax.rem(dev, p.n_y)

    def sub_row(bits, count):
        start = 0
        for s in range(count):
            start = start + bits[s] * p.sizes[s]
        return start

    def first_token(dev):
        bits = mine[:-1] + [lax.rem(lax.div(dev, p.n_y), 2)]
        return group_of(dev) * p.group_tokens + sub_row(bits, p.n_steps)

    def partner(s):
        if s < p.n_steps - 1:
            return r, flip(j, p.cb_bits[s])
        return flip(r, p.n_y), j

    def copy(src, dst, ssem, rsem, dev):
        return pltpu.make_async_remote_copy(
            src_ref=src,
            dst_ref=dst,
            send_sem=ssem,
            recv_sem=rsem,
            device_id=dev,
            device_id_type=MESH,
        )

    def at_rows(start, size):
        return pl.ds(pl.multiple_of(start, size), size)

    own_row = sub_row(mine, p.n_steps)
    own_rows = at_rows(own_row, p.own)
    my_slab = at_rows(r * p.rows, p.rows)

    barrier = pltpu.get_barrier_semaphore()
    for off in range(1, p.n_ra):
        pl.semaphore_signal(barrier, inc=1, device_id=(flip(r, off), j), device_id_type=MESH)
    for bit in p.cb_bits:
        pl.semaphore_signal(barrier, inc=1, device_id=(r, flip(j, bit)), device_id_type=MESH)

    def load(k):
        layer, kind = k // 3, k % 3
        source = (up_w, gate_w, down_w)[kind]
        return pltpu.make_async_copy(source.at[layer], stage.at[k % 2], sem["stage"].at[k % 2])

    load(0).start()
    load(1).start()
    own_tokens = pltpu.make_async_copy(
        tin.at[at_rows(first_token(r), p.own)], tok.at[r], sem["local"].at[0]
    )
    own_tokens.start()
    group = group_of(r)

    def extra_rows(dev):
        return at_rows(group_of(dev) * p.group_tokens - p.extra, p.extra)

    own_extra = pltpu.make_async_copy(tin.at[extra_rows(r)], tok_e.at[r], sem["local"].at[1])

    @pl.when(group > 0)
    def _():
        own_extra.start()

    def token_send(off):
        dev = flip(r, off)
        return copy(
            tin.at[at_rows(first_token(dev), p.own)],
            tok.at[r],
            sem["tok_s"].at[off],
            sem["tok_r"].at[r],
            (dev, j),
        )


    def extra_send(off):
        dev = flip(r, off)
        return copy(
            tin.at[extra_rows(dev)],
            tok_e.at[r],
            sem["toke_s"].at[off],
            sem["toke_r"].at[r],
            (dev, j),
        )

    def slab(k, dev):
        return w.at[k, at_rows(dev * p.rows, p.rows)]

    def z_send(k, dz):
        source = give.at[k] if dz % 2 else slab(k, r)
        return copy(
            source, slab(k, r), sem["z"].at[k, dz], sem["w"].at[k, r], (flip(z, dz) * p.n_y + y, j)
        )

    def y_send(k, dz, dy):
        dev = flip(z, dz) * p.n_y + y
        return copy(
            slab(k, dev),
            slab(k, dev),
            sem["y"].at[k, dz, dy],
            sem["w"].at[k, dev],
            (z * p.n_y + flip(y, dy), j),
        )

    def slab_wait(k, dev):
        copy(slab(k, dev), slab(k, dev), sem["z"].at[k, 0], sem["w"].at[k, dev], (r, j)).wait_recv()

    def forward(k, dz):
        if dz:
            slab_wait(k, flip(z, dz) * p.n_y + y)
        for dy in range(1, p.n_y):
            y_send(k, dz, dy).start()

    def convert(k):
        load(k).wait()
        tile = min(64, p.rows)

        @pl.loop(0, p.rows // tile)
        def _(t):
            rows = at_rows(t * tile, tile)
            keep = stage[k % 2, rows, pl.ds(pl.multiple_of(m * p.half, 128), p.half)]
            rest = stage[k % 2, rows, pl.ds(pl.multiple_of((1 - m) * p.half, 128), p.half)]
            w[k, at_rows(r * p.rows + t * tile, tile), :] = keep.astype(jnp.bfloat16)
            give[k, rows, :] = rest.astype(jnp.bfloat16)

        if k + 2 < n_k:
            load(k + 2).start()

    far = list(range(2, p.n_z))

    def is_inner(plane):
        return jnp.logical_and(plane > 0, plane < p.n_z - 1)

    def far_send(k):
        for wanted in (True, False):
            for dz in far:

                @pl.when(is_inner(flip(z, dz)) == wanted)
                def _():
                    z_send(k, dz).start()

    inner = is_inner(z)

    def block_rows(a):
        count = p.n_steps - a
        size = p.own << a
        return sub_row(mine, count), size

    def gather_copy(layer, a, lanes, ssem, rsem):
        start, size = block_rows(a)
        ref = st.at[layer, at_rows(start, size), lanes]
        return copy(ref, ref, ssem, rsem, partner(p.n_steps - 1 - a))

    def gather_wait(layer, a, lanes, ssem, rsem):
        start, size = block_rows(a)
        s = p.n_steps - 1 - a
        ref = st.at[layer, at_rows(start + (1 - 2 * mine[s]) * size, size), lanes]
        copy(ref, ref, ssem, rsem, (r, j)).wait_recv()

    everything = pl.ds(0, p.features)

    def gather0(a):
        return gather_copy(0, a, everything, sem["g0_s"].at[a], sem["g0_r"].at[a])

    def gather0_wait(a):
        gather_wait(0, a, everything, sem["g0_s"].at[a], sem["g0_r"].at[a])

    convert(0)
    convert(1)
    with jax.named_scope("barrier"):
        pl.semaphore_wait(barrier, p.n_ra - 1 + len(p.cb_bits))
    for off in range(1, p.n_ra):
        token_send(off).start()

        @pl.when(group_of(flip(r, off)) > 0)
        def _():
            extra_send(off).start()

    forward(0, 0)
    forward(1, 0)
    convert(2)
    with jax.named_scope("tokens"):
        own_tokens.wait()
        for src in range(p.n_ra):
            lanes = slice(src * p.rows, (src + 1) * p.rows)

            @pl.when(r != src)
            def _():
                copy(
                    tok.at[src], tok.at[src], sem["tok_s"].at[0], sem["tok_r"].at[src], (r, j)
                ).wait_recv()

            st[0, own_rows, lanes] = tok[src]

    convert(3)
    gather0(0).start()
    z_send(0, 1).start()
    z_send(1, 1).start()

    @pl.when(group > 0)
    def _():
        own_extra.wait()
        for src in range(p.n_ra):

            @pl.when(r != src)
            def _():
                copy(
                    tok_e.at[src], tok_e.at[src], sem["toke_s"].at[0], sem["toke_r"].at[src], (r, j)
                ).wait_recv()

            st_e[:, src * p.rows : (src + 1) * p.rows] = tok_e[src]
        values = st_e[...].astype(jnp.float32)
        total = None
        for c in range(p.features // 128):
            part = values[:, c * 128 : (c + 1) * 128]
            total = part * part if total is None else total + part * part
        sq_e[...] = total

    far_send(0)
    forward(2, 0)
    convert(4)
    convert(5)
    for a in range(p.n_steps):
        with jax.named_scope(f"gather0#a={a}"):
            gather0_wait(a)
        if a + 1 < p.n_steps:
            gather0(a + 1).start()
        if a == 0:
            far_send(1)
            z_send(2, 1).start()
            z_send(3, 1).start()
        if a == 1:
            far_send(2)
            z_send(4, 1).start()
            z_send(5, 1).start()
        if a < 2:
            with jax.named_scope(f"near#k={a}"):
                forward(a, 1)
        if a == 1:
            for dz in far:
                forward(0, dz)

    def chunk_of(i):
        base = (z - m) * p.cy + lax.div(y, p.q)
        total = 0
        shift = 1
        for bit in p.order_bits:
            total = total + lax.rem(lax.div(base, bit) + lax.div(i, shift), 2) * bit
            shift *= 2
        return total

    def chunk_lanes(f):
        return pl.ds(pl.multiple_of(f * p.chunk, p.chunk), p.chunk)

    def chunk_wait(k, f):
        for t in range(p.q):
            dev = f * p.q + t

            @pl.when(lax.rem(dev, p.n_y) != y)
            def _():
                slab_wait(k, dev)

    tile = min(256, p.group_tokens)
    fine = 64

    def squares(layer, lanes, first):
        @pl.loop(0, p.group_tokens // fine)
        def _(t):
            rows = at_rows(t * fine, fine)
            values = st[layer, rows, lanes].astype(jnp.float32)
            total = None
            for c in range(p.chunk // 128):
                part = values[:, c * 128 : (c + 1) * 128]
                total = part * part if total is None else total + part * part
            if first is None:
                sq[rows, :] = sq[rows, :] + total
            else:

                @pl.when(first)
                def _():
                    sq[rows, :] = total

                @pl.when(jnp.logical_not(first))
                def _():
                    sq[rows, :] = sq[rows, :] + total

    @pl.loop(0, p.n_chunks)
    def _(i):
        squares(0, chunk_lanes(i), i == 0)

    def product_chunk(layer, k, dst, i, first):
        f = chunk_of(i)
        chunk_wait(k, f)
        lanes = chunk_lanes(f)
        weights = w.at[k, at_rows(f * p.chunk, p.chunk)]

        @pl.loop(0, p.group_tokens // tile)
        def _(t):
            rows = at_rows(t * tile, tile)
            scaled = st[layer, rows, lanes].astype(jnp.float32) * gain[layer : layer + 1, lanes]
            term = jnp.dot(
                scaled.astype(jnp.bfloat16), weights[...], preferred_element_type=jnp.float32
            )
            to = pl.ds(pl.multiple_of(p.edge + t * tile, 8), tile)
            dst[to, :] = term if first else dst[to, :] + term

        if layer == 0:

            @pl.when(group > 0)
            def _():
                scaled = st_e[:, lanes].astype(jnp.float32) * gain[layer : layer + 1, lanes]
                term = jnp.dot(
                    scaled.astype(jnp.bfloat16), weights[...], preferred_element_type=jnp.float32
                )
                to = (up_e, gate_e)[k % 3]
                to[...] = term if first else to[...] + term

    def product(layer, k, dst):
        product_chunk(layer, k, dst, 0, True)

        @pl.loop(1, p.n_chunks)
        def _(i):
            product_chunk(layer, k, dst, i, False)

    def product_stage(layer, k, dst, i):
        @pl.when(i == 0)
        def _():
            product_chunk(layer, k, dst, i, True)

        @pl.when(i > 0)
        def _():
            product_chunk(layer, k, dst, i, False)

    own_half = pl.ds(pl.multiple_of(m * p.half, 128), p.half)
    following = group + 1
    following_dev = (lax.div(following, p.n_y) * 2 + m) * p.n_y + lax.rem(following, p.n_y)

    def halo_copy(layer, which):
        source = (up, gate)[which]
        return copy(
            source.at[pl.ds(p.group_tokens, p.edge)],
            halo.at[layer, which],
            sem["h_s"].at[layer, which],
            sem["h_r"].at[layer, which],
            (following_dev, j),
        )

    def convolve(layer, between=None):
        scale_u = up_scale[layer : layer + 1, own_half]
        scale_g = gate_scale[layer : layer + 1, own_half]

        @pl.loop(0, p.group_tokens // fine)
        def _(t):
            total = jnp.sum(sq[at_rows(t * fine, fine), :], axis=1, keepdims=True)
            inverse = lax.rsqrt(total * (1.0 / p.features) + EPS)
            rows = pl.ds(pl.multiple_of(p.edge + t * fine, 8), fine)
            up[rows, :] = up[rows, :] * inverse * scale_u
            gate[rows, :] = gate[rows, :] * inverse * scale_g

        if layer:

            @pl.when(following < p.groups)
            def _():
                halo_copy(layer, 0).start()
                halo_copy(layer, 1).start()

            between()

        @pl.when(group > 0)
        def _():
            if layer:
                for which, dst in ((0, up), (1, gate)):
                    copy(
                        halo.at[layer, which],
                        halo.at[layer, which],
                        sem["h_s"].at[layer, which],
                        sem["h_r"].at[layer, which],
                        (r, j),
                    ).wait_recv()
                    dst[0 : p.edge, :] = halo[layer, which]
            else:
                total = jnp.sum(sq_e[...], axis=1, keepdims=True)
                inverse = lax.rsqrt(total * (1.0 / p.features) + EPS)
                up_values = up_e[...] * inverse * scale_u
                gate_values = gate_e[...] * inverse * scale_g
                up[0 : p.edge, :] = up_values[p.extra - p.edge :]
                gate[0 : p.edge, :] = gate_values[p.extra - p.edge :]

        @pl.when(group == 0)
        def _():
            up[0 : p.edge, :] = jnp.zeros((p.edge, p.half), jnp.float32)
            gate[0 : p.edge, :] = jnp.zeros((p.edge, p.half), jnp.float32)

        taps_u = up_taps[:, layer, own_half]
        taps_g = gate_taps[:, layer, own_half]

        def taps_over(ref, taps, t):
            values = ref[pl.ds(pl.multiple_of(t * fine, 8), fine + p.edge), :]
            low = p.edge + 1 - p.width
            total = taps[0:1] * values[low : low + fine]
            for c in range(1, p.width):
                total = total + taps[c : c + 1] * values[low + c : low + c + fine]
            return total

        @pl.loop(0, p.group_tokens // fine)
        def _(t):
            conv_gate = taps_over(gate, taps_g, t)
            conv_up = taps_over(up, taps_u, t)
            value = conv_gate / (1.0 + jnp.exp(-conv_gate)) * conv_up
            hid[at_rows(t * fine, fine), :] = value.astype(jnp.bfloat16)

    def reduce_copy(layer, s, i):
        return copy(
            snds[s].at[i],
            rcvs[s].at[layer, i],
            sem["r_s"].at[layer, s, i],
            sem["r_r"].at[layer, s, i],
            partner(s),
        )

    def reduce_wait(layer, s, i):
        ref = rcvs[s].at[layer, i]
        copy(ref, ref, sem["r_s"].at[layer, s, i], sem["r_r"].at[layer, s, i], (r, j)).wait_recv()

    def down_stage(layer, i):
        k = 3 * layer + 2
        f = chunk_of(i)
        chunk_wait(k, f)
        weights = w.at[k, at_rows(f * p.chunk, p.chunk)]
        size = p.sizes[0]
        step = min(tile, size)

        def term(start):
            return lax.dot_general(
                hid[pl.ds(pl.multiple_of(start, step), step), :],
                weights[...],
                (((1,), (1,)), ((), ())),
                preferred_element_type=jnp.float32,
            )

        @pl.loop(0, size // step)
        def _(t):
            rows = at_rows(t * step, step)
            snds[0][i, rows, :] = term((1 - mine[0]) * size + t * step).astype(jnp.bfloat16)

        @pl.loop(0, size // step)
        def _(t):
            accs[0][lax.rem(i, p.slots), at_rows(t * step, step), :] = term(mine[0] * size + t * step)

        reduce_copy(layer, 0, i).start()

    def reduce_stage(layer, s, i):
        reduce_wait(layer, s - 1, i)
        size = p.sizes[s]
        give_rows = at_rows((1 - mine[s]) * size, size)
        keep_rows = at_rows(mine[s] * size, size)
        arrived = rcvs[s - 1][layer, i, give_rows, :].astype(jnp.float32)
        slot = lax.rem(i, p.slots)
        snds[s][i] = (accs[s - 1][slot, give_rows, :] + arrived).astype(jnp.bfloat16)
        arrived = rcvs[s - 1][layer, i, keep_rows, :].astype(jnp.float32)
        accs[s][slot] = accs[s - 1][slot, keep_rows, :] + arrived
        reduce_copy(layer, s, i).start()

    def gather1(a, f):
        return gather_copy(1, a, chunk_lanes(f), sem["g_s"].at[a, f], sem["g_r"].at[a, f])

    def gather1_wait(a, f):
        gather_wait(1, a, chunk_lanes(f), sem["g_s"].at[a, f], sem["g_r"].at[a, f])

    def out_copy(f, t):
        return copy(
            ost.at[f, t],
            obuf.at[at_rows(first_token(r), p.own)],
            sem["o_s"].at[f, t],
            sem["o_r"].at[r],
            (f * p.q + t, j),
        )

    def last_stage(layer, i):
        f = chunk_of(i)
        s = p.n_steps - 1
        reduce_wait(layer, s, i)
        lanes = chunk_lanes(f)
        total = accs[s][lax.rem(i, p.slots)] + rcvs[s][layer, i].astype(jnp.float32)
        before = st[layer, own_rows, lanes].astype(jnp.float32)
        value = total * down_scale[layer : layer + 1, lanes] + RESIDUAL * before
        value = value.astype(jnp.bfloat16)
        if layer + 1 < p.layers:
            st[layer + 1, own_rows, lanes] = value
            gather1(0, f).start()
        else:
            for t in range(p.q):
                ost[f, t] = value[:, t * p.rows : (t + 1) * p.rows]
                dev = f * p.q + t

                @pl.when(dev == r)
                def _():
                    obuf[at_rows(first_token(r), p.own), :] = ost[f, t]

                @pl.when(dev != r)
                def _():
                    out_copy(f, t).start()

    def gather_stage(a, i):
        f = chunk_of(i)
        gather1_wait(a, f)
        if a + 1 < p.n_steps:
            gather1(a + 1, f).start()
        else:
            squares(1, chunk_lanes(f), i == 0)
            product_stage(1, 3, up, i)

    def pipeline(stages, tasks):
        count = p.n_chunks + stages[-1][0]

        @pl.loop(0, count)
        def _(it):
            for back, (lag, stage) in reversed(list(enumerate(stages))):
                i = it - lag

                @pl.when(jnp.logical_and(i >= 0, i < p.n_chunks))
                def _():
                    with jax.named_scope(f"stage#b={back}"):
                        stage(i)

            for when, task in tasks:

                @pl.when(it == when)
                def _():
                    task()

    sources = [
        (pz, py)
        for pz in range(0, p.n_z, 2)
        for py in range(p.n_y)
    ]
    n_out = p.n_steps - 1

    def out_rows(index, a, flipped):
        pz, py = sources[index]
        dev = flip(z, pz) * p.n_y + flip(y, py)
        start, size = block_rows(a)
        if flipped:
            start = start + (1 - 2 * mine[p.n_steps - 1 - a]) * size
        return obuf.at[at_rows(group_of(dev) * p.group_tokens + start, size)]

    def out_gather(index, a):
        ref = out_rows(index, a, False)
        return copy(
            ref,
            ref,
            sem["oa_s"].at[a - 1, index],
            sem["oa_r"].at[a - 1, index],
            partner(p.n_steps - 1 - a),
        )

    def out_first(index):
        pz, py = sources[index]
        for low in range(2):
            dev = flip(z - m + low, pz) * p.n_y + flip(y, py)

            @pl.when(dev != r)
            def _():
                with jax.named_scope(f"out0#i={index}"):
                    ref = obuf.at[at_rows(first_token(dev), p.own)]
                    copy(ref, ref, sem["o_s"].at[0, 0], sem["o_r"].at[dev], (r, j)).wait_recv()

        out_gather(index, 1).start()

    def halo_done(layer):
        @pl.when(following < p.groups)
        def _():
            halo_copy(layer, 0).wait_send()
            halo_copy(layer, 1).wait_send()

    def far_forward(k):
        with jax.named_scope(f"far#k={k}"):
            for dz in far:
                forward(k, dz)

    def near_forward(k):
        with jax.named_scope(f"near#k={k}"):
            forward(k, 1)

    for layer in range(p.layers):
        last = layer + 1 == p.layers
        k = 3 * layer
        if layer == 0:
            far_send(3)
            with jax.named_scope(f"up#l={layer}"):
                product(layer, k, up)
            far_forward(1)
            near_forward(2)
            forward(3, 0)
        if layer:
            far_forward(4)
        with jax.named_scope(f"gate#l={layer}"):
            product(layer, k + 1, gate)
        with jax.named_scope(f"convolve#l={layer}"):
            convolve(layer, lambda: None)
        if layer == 0:

            @pl.when(inner)
            def _():
                far_send(4)
                far_send(5)

        stages = [(0, functools.partial(down_stage, layer))]
        lag = 1
        for step in range(1, p.n_steps):
            stages.append((lag, functools.partial(reduce_stage, layer, step)))
            lag += 2
        stages.append((lag, functools.partial(last_stage, layer)))
        tasks = []
        if not last:
            for step in range(p.n_steps):
                lag += 2 if step + 1 < p.n_steps else 1
                stages.append((lag, functools.partial(gather_stage, step)))

            def outer_send(k):
                @pl.when(jnp.logical_not(inner))
                def _():
                    far_send(k)

            tasks = [
                (1, lambda: far_forward(2)),
                (2, lambda: near_forward(3)),
                (2, lambda: forward(4, 0)),
                (3, lambda: near_forward(4)),
                (3, lambda: forward(5, 0)),
                (5, lambda: near_forward(5)),
                (8, lambda: outer_send(4)),
                (10, lambda: far_forward(3)),
                (13, lambda: outer_send(5)),
            ]
        else:
            tasks = [(3, lambda: far_forward(5))]
            count = p.n_chunks + lag
            early = [index for index in range(p.groups) if p.q == 1 and 2 * index + 4 + lag < count]
            tasks += [
                (2 * index + 4 + lag, functools.partial(out_first, index)) for index in early
            ]
        with jax.named_scope(f"down#l={layer}"):
            pipeline(stages, tasks)

        @pl.loop(0, p.n_chunks)
        def _(i):
            for s in range(p.n_steps):
                reduce_copy(layer, s, i).wait_send()

        if last:
            halo_done(layer)

    for index in range(len(sources)):
        if index not in early:
            out_first(index)
    for a in range(1, p.n_steps):
        for index in range(len(sources)):
            ref = out_rows(index, a, True)
            with jax.named_scope(f"out{a}#i={index}"):
                copy(
                    ref, ref, sem["oa_s"].at[a - 1, index], sem["oa_r"].at[a - 1, index], (r, j)
                ).wait_recv()
            if a + 1 < p.n_steps:
                out_gather(index, a + 1).start()

    result = pltpu.make_async_copy(obuf, out, sem["local"].at[0])
    result.start()
    finish = jax.named_scope("finish")
    finish.__enter__()
    for off in range(1, p.n_ra):
        token_send(off).wait_send()

        @pl.when(group_of(flip(r, off)) > 0)
        def _():
            extra_send(off).wait_send()

    for k in range(n_k):
        for dz in range(1, p.n_z):
            z_send(k, dz).wait_send()
        for dz in range(p.n_z):
            for dy in range(1, p.n_y):
                y_send(k, dz, dy).wait_send()
    for a in range(p.n_steps):
        gather0(a).wait_send()

    @pl.loop(0, p.n_chunks)
    def _(f):
        for a in range(p.n_steps):
            gather1(a, f).wait_send()
        for t in range(p.q):

            @pl.when(f * p.q + t != r)
            def _():
                out_copy(f, t).wait_send()

    for a in range(1, p.n_steps):
        for index in range(len(sources)):
            out_gather(index, a).wait_send()
    result.wait()
    finish.__exit__(None, None, None)


def per_device(
    tokens,
    norm_gain,
    up_weight,
    gate_weight,
    up_scale,
    gate_scale,
    up_taps,
    gate_taps,
    down_weight,
    down_scale,
):
    layers, rows, columns = up_weight.shape
    p = Plan(
        lax.axis_size("ra"),
        lax.axis_size("cb"),
        rows,
        columns,
        tokens.shape[1],
        layers,
        up_taps.shape[1],
    )
    n_k = 3 * layers
    bf16, f32 = jnp.bfloat16, jnp.float32
    dma = pltpu.SemaphoreType.DMA
    in_hbm = pl.BlockSpec(memory_space=pl.ANY)
    in_vmem = pl.BlockSpec(memory_space=pltpu.VMEM)
    sems = {
        "stage": dma((2,)),
        "local": dma((2,)),
        "tok_s": dma((p.n_ra,)),
        "tok_r": dma((p.n_ra,)),
        "toke_s": dma((p.n_ra,)),
        "toke_r": dma((p.n_ra,)),
        "w": dma((n_k, p.n_ra)),
        "z": dma((n_k, p.n_z)),
        "y": dma((n_k, p.n_z, p.n_y)),
        "g0_s": dma((p.n_steps,)),
        "g0_r": dma((p.n_steps,)),
        "g_s": dma((p.n_steps, p.n_chunks)),
        "g_r": dma((p.n_steps, p.n_chunks)),
        "r_s": dma((layers, p.n_steps, p.n_chunks)),
        "r_r": dma((layers, p.n_steps, p.n_chunks)),
        "h_s": dma((layers, 2)),
        "h_r": dma((layers, 2)),
        "o_s": dma((p.n_chunks, p.q)),
        "o_r": dma((p.n_ra,)),
        "oa_s": dma((p.n_steps - 1, p.groups)),
        "oa_r": dma((p.n_steps - 1, p.groups)),
    }
    names = list(sems)
    n_s = p.n_steps

    def body(*refs):
        head, rest = refs[: 11 + 17], refs[11 + 17 :]
        accs, snds, rcvs = rest[:n_s], rest[n_s : 2 * n_s], rest[2 * n_s : 3 * n_s]
        kernel(p, *head, accs, snds, rcvs, dict(zip(names, rest[3 * n_s :])))

    turned = pl.pallas_call(
        body,
        out_shape=jax.ShapeDtypeStruct((p.length, rows), bf16),
        in_specs=[in_hbm] * 4 + [in_vmem] * 6,
        out_specs=in_hbm,
        scratch_shapes=[
            pltpu.VMEM((n_k, p.features, p.half), bf16),
            pltpu.VMEM((n_k, rows, p.half), bf16),
            pltpu.VMEM((2, rows, columns), f32),
            pltpu.VMEM((layers, p.group_tokens, p.features), bf16),
            pltpu.VMEM((p.edge + p.group_tokens, p.half), f32),
            pltpu.VMEM((p.edge + p.group_tokens, p.half), f32),
            pltpu.VMEM((p.group_tokens, p.half), bf16),
            pltpu.VMEM((p.n_ra, p.own, rows), bf16),
            pltpu.VMEM((p.n_ra, p.extra, rows), bf16),
            pltpu.VMEM((p.extra, p.features), bf16),
            pltpu.VMEM((p.extra, p.half), f32),
            pltpu.VMEM((p.extra, p.half), f32),
            pltpu.VMEM((p.extra, 128), f32),
            pltpu.VMEM((p.group_tokens, 128), f32),
            pltpu.VMEM((layers, 2, p.edge, p.half), f32),
            pltpu.VMEM((p.length, rows), bf16),
            pltpu.VMEM((p.n_chunks, p.q, p.own, rows), bf16),
        ]
        + [pltpu.VMEM((p.slots, size, p.chunk), f32) for size in p.sizes]
        + [pltpu.VMEM((p.n_chunks, size, p.chunk), bf16) for size in p.sizes]
        + [pltpu.VMEM((layers, p.n_chunks, size, p.chunk), bf16) for size in p.sizes]
        + [sems[name] for name in names],
        compiler_params=pltpu.CompilerParams(
            collective_id=0, has_side_effects=True, vmem_limit_bytes=66 * 1000 * 1000
        ),
        name="layers",
    )(
        tokens.T,
        up_weight,
        gate_weight,
        down_weight,
        norm_gain,
        up_scale,
        gate_scale,
        jnp.swapaxes(up_taps, 0, 1),
        jnp.swapaxes(gate_taps, 0, 1),
        down_scale,
    )
    return turned.T


def solution(mesh):
    placed = (
        P("ra", None),
        P(),
        P(None, "ra", "cb"),
        P(None, "ra", "cb"),
        P(None, "cb"),
        P(None, "cb"),
        P(None, None, "cb"),
        P(None, None, "cb"),
        P(None, "ra", "cb"),
        P(),
    )
    return jax.shard_map(
        per_device, mesh=mesh, in_specs=placed, out_specs=P("ra", None), check_vma=False
    )
```

```python
import functools

import jax
import jax.numpy as jnp
from jax import lax
from jax.experimental import pallas as pl
from jax.experimental.pallas import tpu as pltpu
from jax.sharding import PartitionSpec as P

EPS = 1e-06
RESIDUAL = 0.5
MESH = pl.DeviceIdType.MESH


def doublings(low, high):
    bits = []
    while low < high:
        bits.append(low)
        low *= 2
    return bits


def bit_of(value, bit):
    return lax.rem(lax.div(value, bit), 2) if not isinstance(value, int) else (value // bit) % 2


def flip(value, offset):
    for bit in doublings(1, offset + 1):
        if offset & bit:
            value = value + bit - 2 * bit * bit_of(value, bit)
    return value


class Plan:
    def __init__(self, n_ra, n_cb, rows, columns, length, layers, width):
        self.n_ra, self.n_cb, self.rows, self.columns = n_ra, n_cb, rows, columns
        self.length, self.layers, self.width = length, layers, width
        self.n_y = 1 << ((n_ra.bit_length() - 1) // 2)
        self.n_z = n_ra // self.n_y
        self.half = columns // 2
        self.groups = n_ra // 2
        self.group_tokens = length // self.groups
        self.cb_bits = doublings(1, n_cb)
        self.n_steps = len(self.cb_bits) + 1
        self.sizes = [self.group_tokens >> (s + 1) for s in range(self.n_steps)]
        self.own = self.sizes[-1]
        self.q = 1
        while rows * self.q < 256 and self.q < self.n_y:
            self.q *= 2
        self.chunk = rows * self.q
        self.n_chunks = n_ra // self.q
        self.features = n_ra * rows
        cy = self.n_y // self.q
        self.cy = cy
        self.order_bits = [cy] + doublings(1, cy) + doublings(2 * cy, self.n_z * cy)
        self.edge = 8
        self.extra = 16
        self.slots = 3


def kernel(
    p,
    tin,
    up_w,
    gate_w,
    down_w,
    gain,
    up_scale,
    gate_scale,
    up_taps,
    gate_taps,
    down_scale,
    out,
    w,
    give,
    stage,
    st,
    up,
    gate,
    hid,
    tok,
    tok_e,
    st_e,
    up_e,
    gate_e,
    sq_e,
    sq,
    tail,
    halo,
    obuf,
    ost,
    accs,
    snds,
    rcvs,
    sem,
):
    r, j = lax.axis_index("ra"), lax.axis_index("cb")
    z, y = lax.div(r, p.n_y), lax.rem(r, p.n_y)
    m = lax.rem(z, 2)
    mine = [bit_of(j, bit) for bit in p.cb_bits] + [m]
    n_k = 3 * p.layers

    def group_of(dev):
        return lax.div(lax.div(dev, p.n_y), 2) * p.n_y + lax.rem(dev, p.n_y)

    def sub_row(bits, count):
        start = 0
        for s in range(count):
            start = start + bits[s] * p.sizes[s]
        return start

    def first_token(dev):
        bits = mine[:-1] + [lax.rem(lax.div(dev, p.n_y), 2)]
        return group_of(dev) * p.group_tokens + sub_row(bits, p.n_steps)

    def partner(s):
        if s < p.n_steps - 1:
            return r, flip(j, p.cb_bits[s])
        return flip(r, p.n_y), j

    def copy(src, dst, ssem, rsem, dev):
        return pltpu.make_async_remote_copy(
            src_ref=src,
            dst_ref=dst,
            send_sem=ssem,
            recv_sem=rsem,
            device_id=dev,
            device_id_type=MESH,
        )

    def at_rows(start, size):
        return pl.ds(pl.multiple_of(start, size), size)

    own_row = sub_row(mine, p.n_steps)
    own_rows = at_rows(own_row, p.own)
    my_slab = at_rows(r * p.rows, p.rows)

    barrier = pltpu.get_barrier_semaphore()
    for off in range(1, p.n_ra):
        pl.semaphore_signal(barrier, inc=1, device_id=(flip(r, off), j), device_id_type=MESH)
    for bit in p.cb_bits:
        pl.semaphore_signal(barrier, inc=1, device_id=(r, flip(j, bit)), device_id_type=MESH)

    def load(k):
        layer, kind = k // 3, k % 3
        source = (up_w, gate_w, down_w)[kind]
        return pltpu.make_async_copy(source.at[layer], stage.at[k % 2], sem["stage"].at[k % 2])

    load(0).start()
    load(1).start()
    own_tokens = pltpu.make_async_copy(
        tin.at[at_rows(first_token(r), p.own)], tok.at[r], sem["local"].at[0]
    )
    own_tokens.start()
    group = group_of(r)

    def extra_rows(dev):
        return at_rows(group_of(dev) * p.group_tokens - p.extra, p.extra)

    own_extra = pltpu.make_async_copy(tin.at[extra_rows(r)], tok_e.at[r], sem["local"].at[1])

    @pl.when(group > 0)
    def _():
        own_extra.start()

    def token_send(off):
        dev = flip(r, off)
        return copy(
            tin.at[at_rows(first_token(dev), p.own)],
            tok.at[r],
            sem["tok_s"].at[off],
            sem["tok_r"].at[r],
            (dev, j),
        )


    def extra_send(off):
        dev = flip(r, off)
        return copy(
            tin.at[extra_rows(dev)],
            tok_e.at[r],
            sem["toke_s"].at[off],
            sem["toke_r"].at[r],
            (dev, j),
        )

    def slab(k, dev):
        return w.at[k, at_rows(dev * p.rows, p.rows)]

    def z_send(k, dz):
        source = give.at[k] if dz % 2 else slab(k, r)
        return copy(
            source, slab(k, r), sem["z"].at[k, dz], sem["w"].at[k, r], (flip(z, dz) * p.n_y + y, j)
        )

    def y_send(k, dz, dy):
        dev = flip(z, dz) * p.n_y + y
        return copy(
            slab(k, dev),
            slab(k, dev),
            sem["y"].at[k, dz, dy],
            sem["w"].at[k, dev],
            (z * p.n_y + flip(y, dy), j),
        )

    def slab_wait(k, dev):
        copy(slab(k, dev), slab(k, dev), sem["z"].at[k, 0], sem["w"].at[k, dev], (r, j)).wait_recv()

    def forward(k, dz):
        if dz:
            slab_wait(k, flip(z, dz) * p.n_y + y)
        for dy in range(1, p.n_y):
            y_send(k, dz, dy).start()

    def convert(k):
        load(k).wait()
        tile = min(64, p.rows)

        @pl.loop(0, p.rows // tile)
        def _(t):
            rows = at_rows(t * tile, tile)
            keep = stage[k % 2, rows, pl.ds(pl.multiple_of(m * p.half, 128), p.half)]
            rest = stage[k % 2, rows, pl.ds(pl.multiple_of((1 - m) * p.half, 128), p.half)]
            w[k, at_rows(r * p.rows + t * tile, tile), :] = keep.astype(jnp.bfloat16)
            give[k, rows, :] = rest.astype(jnp.bfloat16)

        if k + 2 < n_k:
            load(k + 2).start()

    far = list(range(2, p.n_z))

    def is_inner(plane):
        return jnp.logical_and(plane > 0, plane < p.n_z - 1)

    def far_send(k):
        if k >= 3:
            for dz in far:
                z_send(k, dz).start()
            return
        for wanted in (True, False):
            for dz in far:

                @pl.when(is_inner(flip(z, dz)) == wanted)
                def _():
                    z_send(k, dz).start()

    inner = is_inner(z)

    def block_rows(a):
        count = p.n_steps - a
        size = p.own << a
        return sub_row(mine, count), size

    def gather_copy(layer, a, lanes, ssem, rsem):
        start, size = block_rows(a)
        ref = st.at[layer, at_rows(start, size), lanes]
        return copy(ref, ref, ssem, rsem, partner(p.n_steps - 1 - a))

    def gather_wait(layer, a, lanes, ssem, rsem):
        start, size = block_rows(a)
        s = p.n_steps - 1 - a
        ref = st.at[layer, at_rows(start + (1 - 2 * mine[s]) * size, size), lanes]
        copy(ref, ref, ssem, rsem, (r, j)).wait_recv()

    everything = pl.ds(0, p.features)

    def gather0(a):
        return gather_copy(0, a, everything, sem["g0_s"].at[a], sem["g0_r"].at[a])

    def gather0_wait(a):
        gather_wait(0, a, everything, sem["g0_s"].at[a], sem["g0_r"].at[a])

    convert(0)
    convert(1)
    with jax.named_scope("barrier"):
        pl.semaphore_wait(barrier, p.n_ra - 1 + len(p.cb_bits))
    for off in range(1, p.n_ra):
        token_send(off).start()

        @pl.when(group_of(flip(r, off)) > 0)
        def _():
            extra_send(off).start()

    forward(0, 0)
    forward(1, 0)
    convert(2)
    with jax.named_scope("tokens"):
        own_tokens.wait()
        for src in range(p.n_ra):
            lanes = slice(src * p.rows, (src + 1) * p.rows)

            @pl.when(r != src)
            def _():
                copy(
                    tok.at[src], tok.at[src], sem["tok_s"].at[0], sem["tok_r"].at[src], (r, j)
                ).wait_recv()

            st[0, own_rows, lanes] = tok[src]

    convert(3)
    gather0(0).start()
    z_send(0, 1).start()
    z_send(1, 1).start()

    @pl.when(group > 0)
    def _():
        own_extra.wait()
        for src in range(p.n_ra):

            @pl.when(r != src)
            def _():
                copy(
                    tok_e.at[src], tok_e.at[src], sem["toke_s"].at[0], sem["toke_r"].at[src], (r, j)
                ).wait_recv()

            st_e[:, src * p.rows : (src + 1) * p.rows] = tok_e[src]
        values = st_e[...].astype(jnp.float32)
        total = None
        for c in range(p.features // 128):
            part = values[:, c * 128 : (c + 1) * 128]
            total = part * part if total is None else total + part * part
        sq_e[...] = total

    far_send(0)
    forward(2, 0)
    convert(4)
    convert(5)
    for a in range(p.n_steps):
        with jax.named_scope(f"gather0#a={a}"):
            gather0_wait(a)
        if a + 1 < p.n_steps:
            gather0(a + 1).start()
        if a == 0:
            far_send(1)
            z_send(2, 1).start()
            z_send(3, 1).start()
        if a == 1:
            far_send(2)
            z_send(4, 1).start()
            z_send(5, 1).start()
        if a < 2:
            with jax.named_scope(f"near#k={a}"):
                forward(a, 1)
        if a == 1:
            for dz in far:
                forward(0, dz)

    def chunk_of(i):
        base = (z - m) * p.cy + lax.div(y, p.q)
        total = 0
        shift = 1
        for bit in p.order_bits:
            total = total + lax.rem(lax.div(base, bit) + lax.div(i, shift), 2) * bit
            shift *= 2
        return total

    def chunk_lanes(f):
        return pl.ds(pl.multiple_of(f * p.chunk, p.chunk), p.chunk)

    def chunk_wait(k, f):
        for t in range(p.q):
            dev = f * p.q + t

            @pl.when(lax.rem(dev, p.n_y) != y)
            def _():
                slab_wait(k, dev)

    tile = min(256, p.group_tokens)
    fine = 64

    def squares(layer, lanes, first):
        @pl.loop(0, p.group_tokens // fine)
        def _(t):
            rows = at_rows(t * fine, fine)
            values = st[layer, rows, lanes].astype(jnp.float32)
            total = None
            for c in range(p.chunk // 128):
                part = values[:, c * 128 : (c + 1) * 128]
                total = part * part if total is None else total + part * part
            if first is None:
                sq[rows, :] = sq[rows, :] + total
            else:

                @pl.when(first)
                def _():
                    sq[rows, :] = total

                @pl.when(jnp.logical_not(first))
                def _():
                    sq[rows, :] = sq[rows, :] + total

    @pl.loop(0, p.n_chunks)
    def _(i):
        squares(0, chunk_lanes(i), i == 0)

    def product_chunk(layer, k, dst, i, first):
        f = chunk_of(i)
        chunk_wait(k, f)
        lanes = chunk_lanes(f)
        weights = w.at[k, at_rows(f * p.chunk, p.chunk)]

        @pl.loop(0, p.group_tokens // tile)
        def _(t):
            rows = at_rows(t * tile, tile)
            scaled = st[layer, rows, lanes].astype(jnp.float32) * gain[layer : layer + 1, lanes]
            term = jnp.dot(
                scaled.astype(jnp.bfloat16), weights[...], preferred_element_type=jnp.float32
            )
            to = pl.ds(pl.multiple_of(p.edge + t * tile, 8), tile)
            dst[to, :] = term if first else dst[to, :] + term

        if layer == 0:

            @pl.when(group > 0)
            def _():
                scaled = st_e[:, lanes].astype(jnp.float32) * gain[layer : layer + 1, lanes]
                term = jnp.dot(
                    scaled.astype(jnp.bfloat16), weights[...], preferred_element_type=jnp.float32
                )
                to = (up_e, gate_e)[k % 3]
                to[...] = term if first else to[...] + term

    def product(layer, k, dst, start, stop):
        if start == 0:
            product_chunk(layer, k, dst, 0, True)

        @pl.loop(max(start, 1), stop)
        def _(i):
            product_chunk(layer, k, dst, i, False)

    def product_stage(layer, k, dst, i):
        @pl.when(i == 0)
        def _():
            product_chunk(layer, k, dst, i, True)

        @pl.when(i > 0)
        def _():
            product_chunk(layer, k, dst, i, False)

    own_half = pl.ds(pl.multiple_of(m * p.half, 128), p.half)
    following = group + 1
    following_dev = (lax.div(following, p.n_y) * 2 + m) * p.n_y + lax.rem(following, p.n_y)

    def halo_copy(layer, which):
        return copy(
            tail.at[layer, which],
            halo.at[layer, which],
            sem["h_s"].at[layer, which],
            sem["h_r"].at[layer, which],
            (following_dev, j),
        )

    def inverse_of(squares_sum):
        total = jnp.sum(squares_sum, axis=1, keepdims=True)
        return lax.rsqrt(total * (1.0 / p.features) + EPS)

    def convolve(layer, between):
        if layer:
            inverse = inverse_of(sq[p.group_tokens - p.edge : p.group_tokens, :])
            ends = slice(p.group_tokens, p.group_tokens + p.edge)
            tail[layer, 0] = up[ends, :] * inverse
            tail[layer, 1] = gate[ends, :] * inverse

            @pl.when(following < p.groups)
            def _():
                halo_copy(layer, 0).start()
                halo_copy(layer, 1).start()

        taps_u = up_taps[:, layer, own_half] * up_scale[layer : layer + 1, own_half]
        taps_g = gate_taps[:, layer, own_half] * gate_scale[layer : layer + 1, own_half]
        low = p.edge + 1 - p.width

        def taps_over(values, taps):
            total = taps[0:1] * values[low : low + fine]
            for c in range(1, p.width):
                total = total + taps[c : c + 1] * values[low + c : low + c + fine]
            return total

        def finish_tile(up_values, gate_values, t):
            conv_gate = taps_over(gate_values, taps_g)
            conv_up = taps_over(up_values, taps_u)
            value = conv_gate / (1.0 + jnp.exp(-conv_gate)) * conv_up
            hid[at_rows(t * fine, fine), :] = value.astype(jnp.bfloat16)

        tiles = p.group_tokens // fine

        @pl.loop(0, tiles - 1)
        def _(step):
            t = tiles - 1 - step
            before = pl.ds(pl.multiple_of(t * fine - p.edge, 8), fine + p.edge)
            inverse = inverse_of(sq[before, :])
            rows = pl.ds(pl.multiple_of(t * fine, 8), fine + p.edge)
            finish_tile(up[rows, :] * inverse, gate[rows, :] * inverse, t)

        if layer:
            between()

        @pl.when(group > 0)
        def _():
            if layer:
                for which, dst in ((0, up), (1, gate)):
                    copy(
                        halo.at[layer, which],
                        halo.at[layer, which],
                        sem["h_s"].at[layer, which],
                        sem["h_r"].at[layer, which],
                        (r, j),
                    ).wait_recv()
                    dst[0 : p.edge, :] = halo[layer, which]
            else:
                inverse = inverse_of(sq_e[...])[p.extra - p.edge :]
                up[0 : p.edge, :] = up_e[p.extra - p.edge :, :] * inverse
                gate[0 : p.edge, :] = gate_e[p.extra - p.edge :, :] * inverse

        @pl.when(group == 0)
        def _():
            up[0 : p.edge, :] = jnp.zeros((p.edge, p.half), jnp.float32)
            gate[0 : p.edge, :] = jnp.zeros((p.edge, p.half), jnp.float32)

        inverse = inverse_of(sq[0:fine, :])
        first = slice(p.edge, p.edge + fine)
        finish_tile(
            jnp.concatenate([up[0 : p.edge, :], up[first, :] * inverse], axis=0),
            jnp.concatenate([gate[0 : p.edge, :], gate[first, :] * inverse], axis=0),
            0,
        )

    def reduce_copy(layer, s, i):
        return copy(
            snds[s].at[i],
            rcvs[s].at[layer, i],
            sem["r_s"].at[layer, s, i],
            sem["r_r"].at[layer, s, i],
            partner(s),
        )

    def reduce_wait(layer, s, i):
        ref = rcvs[s].at[layer, i]
        copy(ref, ref, sem["r_s"].at[layer, s, i], sem["r_r"].at[layer, s, i], (r, j)).wait_recv()

    def down_stage(layer, i):
        k = 3 * layer + 2
        f = chunk_of(i)
        chunk_wait(k, f)
        weights = w.at[k, at_rows(f * p.chunk, p.chunk)]
        size = p.sizes[0]
        step = min(tile, size)

        def term(start):
            return lax.dot_general(
                hid[pl.ds(pl.multiple_of(start, step), step), :],
                weights[...],
                (((1,), (1,)), ((), ())),
                preferred_element_type=jnp.float32,
            )

        @pl.loop(0, size // step)
        def _(t):
            rows = at_rows(t * step, step)
            snds[0][i, rows, :] = term((1 - mine[0]) * size + t * step).astype(jnp.bfloat16)

        @pl.loop(0, size // step)
        def _(t):
            accs[0][lax.rem(i, p.slots), at_rows(t * step, step), :] = term(mine[0] * size + t * step)

        reduce_copy(layer, 0, i).start()

    def reduce_stage(layer, s, i):
        reduce_wait(layer, s - 1, i)
        size = p.sizes[s]
        slot = lax.rem(i, p.slots)
        give_rows = at_rows((1 - mine[s]) * size, size)
        keep_rows = at_rows(mine[s] * size, size)
        arrived = rcvs[s - 1][layer, i, give_rows, :].astype(jnp.float32)
        snds[s][i] = (accs[s - 1][slot, give_rows, :] + arrived).astype(jnp.bfloat16)
        arrived = rcvs[s - 1][layer, i, keep_rows, :].astype(jnp.float32)
        accs[s][slot] = accs[s - 1][slot, keep_rows, :] + arrived
        reduce_copy(layer, s, i).start()

    def gather1(a, f):
        return gather_copy(1, a, chunk_lanes(f), sem["g_s"].at[a, f], sem["g_r"].at[a, f])

    def gather1_wait(a, f):
        gather_wait(1, a, chunk_lanes(f), sem["g_s"].at[a, f], sem["g_r"].at[a, f])

    def out_copy(f, t):
        return copy(
            ost.at[f, t],
            obuf.at[at_rows(first_token(r), p.own)],
            sem["o_s"].at[f, t],
            sem["o_r"].at[r],
            (f * p.q + t, j),
        )

    def last_stage(layer, i):
        f = chunk_of(i)
        s = p.n_steps - 1
        reduce_wait(layer, s, i)
        lanes = chunk_lanes(f)
        total = accs[s][lax.rem(i, p.slots)] + rcvs[s][layer, i].astype(jnp.float32)
        before = st[layer, own_rows, lanes].astype(jnp.float32)
        value = total * down_scale[layer : layer + 1, lanes] + RESIDUAL * before
        value = value.astype(jnp.bfloat16)
        if layer + 1 < p.layers:
            st[layer + 1, own_rows, lanes] = value
            gather1(0, f).start()
        else:
            for t in range(p.q):
                ost[f, t] = value[:, t * p.rows : (t + 1) * p.rows]
                dev = f * p.q + t

                @pl.when(dev == r)
                def _():
                    obuf[at_rows(first_token(r), p.own), :] = ost[f, t]

                @pl.when(dev != r)
                def _():
                    out_copy(f, t).start()

    def gather_stage(a, i):
        f = chunk_of(i)
        gather1_wait(a, f)
        if a + 1 < p.n_steps:
            gather1(a + 1, f).start()
        else:
            squares(1, chunk_lanes(f), i == 0)
            product_stage(1, 3, up, i)

    def pipeline(stages, tasks):
        count = p.n_chunks + stages[-1][0]

        @pl.loop(0, count)
        def _(it):
            for back, (lag, stage) in reversed(list(enumerate(stages))):
                i = it - lag

                @pl.when(jnp.logical_and(i >= 0, i < p.n_chunks))
                def _():
                    with jax.named_scope(f"stage#b={back}"):
                        stage(i)

            for when, task in tasks:

                @pl.when(it == when)
                def _():
                    task()

    sources = [
        (pz, py)
        for pz in range(0, p.n_z, 2)
        for py in range(p.n_y)
    ]
    n_out = p.n_steps - 1

    def out_rows(index, a, flipped):
        pz, py = sources[index]
        dev = flip(z, pz) * p.n_y + flip(y, py)
        start, size = block_rows(a)
        if flipped:
            start = start + (1 - 2 * mine[p.n_steps - 1 - a]) * size
        return obuf.at[at_rows(group_of(dev) * p.group_tokens + start, size)]

    def out_gather(index, a):
        ref = out_rows(index, a, False)
        return copy(
            ref,
            ref,
            sem["oa_s"].at[a - 1, index],
            sem["oa_r"].at[a - 1, index],
            partner(p.n_steps - 1 - a),
        )

    def out_first(index):
        pz, py = sources[index]
        for low in range(2):
            dev = flip(z - m + low, pz) * p.n_y + flip(y, py)

            @pl.when(dev != r)
            def _():
                with jax.named_scope(f"out0#i={index}"):
                    ref = obuf.at[at_rows(first_token(dev), p.own)]
                    copy(ref, ref, sem["o_s"].at[0, 0], sem["o_r"].at[dev], (r, j)).wait_recv()

        out_gather(index, 1).start()

    def halo_done(layer):
        @pl.when(following < p.groups)
        def _():
            halo_copy(layer, 0).wait_send()
            halo_copy(layer, 1).wait_send()

    def far_forward(k, part=slice(None)):
        with jax.named_scope(f"far#k={k}"):
            for dz in far[part]:
                forward(k, dz)

    def near_forward(k):
        with jax.named_scope(f"near#k={k}"):
            forward(k, 1)

    for layer in range(p.layers):
        last = layer + 1 == p.layers
        k = 3 * layer
        if layer == 0:
            far_send(3)
            with jax.named_scope(f"up#l={layer}"):
                product(layer, k, up, 0, p.n_chunks)
            far_forward(1)
            near_forward(2)
            forward(3, 0)
        with jax.named_scope(f"gate#l={layer}"):
            if layer:
                product(layer, k + 1, gate, 0, p.n_chunks - 2)
                far_forward(5, slice(1))
                product(layer, k + 1, gate, p.n_chunks - 2, p.n_chunks)
            else:
                product(layer, k + 1, gate, 0, p.n_chunks)
        with jax.named_scope(f"convolve#l={layer}"):
            convolve(layer, lambda: far_forward(5, slice(1, None)))
        if layer == 0:

            @pl.when(inner)
            def _():
                far_send(4)
                far_send(5)

        stages = [(0, functools.partial(down_stage, layer))]
        lag = 1
        for step in range(1, p.n_steps):
            stages.append((lag, functools.partial(reduce_stage, layer, step)))
            lag += 2
        stages.append((lag, functools.partial(last_stage, layer)))
        tasks = []
        if not last:
            for step in range(p.n_steps):
                lag += 2 if step + 1 < p.n_steps else 1
                stages.append((lag, functools.partial(gather_stage, step)))

            def outer_send(k):
                @pl.when(jnp.logical_not(inner))
                def _():
                    far_send(k)

            tasks = [
                (1, lambda: far_forward(2)),
                (2, lambda: near_forward(3)),
                (2, lambda: forward(4, 0)),
                (3, lambda: near_forward(4)),
                (3, lambda: forward(5, 0)),
                (5, lambda: near_forward(5)),
                (8, lambda: outer_send(4)),
                (9, lambda: far_forward(3, slice(1))),
                (10, lambda: far_forward(3, slice(1, None))),
                (12, lambda: outer_send(5)),
                (13, lambda: far_forward(4, slice(1))),
                (15, lambda: far_forward(4, slice(1, None))),
            ]
        else:
            count = p.n_chunks + lag
            early = [index for index in range(p.groups) if p.q == 1 and 2 * index + 4 + lag < count]
            tasks += [
                (2 * index + 4 + lag, functools.partial(out_first, index)) for index in early
            ]
        with jax.named_scope(f"down#l={layer}"):
            pipeline(stages, tasks)

        @pl.loop(0, p.n_chunks)
        def _(i):
            for s in range(p.n_steps):
                reduce_copy(layer, s, i).wait_send()

        if last:
            halo_done(layer)

    for index in range(len(sources)):
        if index not in early:
            out_first(index)
    for a in range(1, p.n_steps):
        for index in range(len(sources)):
            ref = out_rows(index, a, True)
            with jax.named_scope(f"out{a}#i={index}"):
                copy(
                    ref, ref, sem["oa_s"].at[a - 1, index], sem["oa_r"].at[a - 1, index], (r, j)
                ).wait_recv()
            if a + 1 < p.n_steps:
                out_gather(index, a + 1).start()

    result = pltpu.make_async_copy(obuf, out, sem["local"].at[0])
    result.start()
    finish = jax.named_scope("finish")
    finish.__enter__()
    for off in range(1, p.n_ra):
        token_send(off).wait_send()

        @pl.when(group_of(flip(r, off)) > 0)
        def _():
            extra_send(off).wait_send()

    for k in range(n_k):
        for dz in range(1, p.n_z):
            z_send(k, dz).wait_send()
        for dz in range(p.n_z):
            for dy in range(1, p.n_y):
                y_send(k, dz, dy).wait_send()
    for a in range(p.n_steps):
        gather0(a).wait_send()

    @pl.loop(0, p.n_chunks)
    def _(f):
        for a in range(p.n_steps):
            gather1(a, f).wait_send()
        for t in range(p.q):

            @pl.when(f * p.q + t != r)
            def _():
                out_copy(f, t).wait_send()

    for a in range(1, p.n_steps):
        for index in range(len(sources)):
            out_gather(index, a).wait_send()
    result.wait()
    finish.__exit__(None, None, None)


def per_device(
    tokens,
    norm_gain,
    up_weight,
    gate_weight,
    up_scale,
    gate_scale,
    up_taps,
    gate_taps,
    down_weight,
    down_scale,
):
    layers, rows, columns = up_weight.shape
    p = Plan(
        lax.axis_size("ra"),
        lax.axis_size("cb"),
        rows,
        columns,
        tokens.shape[1],
        layers,
        up_taps.shape[1],
    )
    n_k = 3 * layers
    bf16, f32 = jnp.bfloat16, jnp.float32
    dma = pltpu.SemaphoreType.DMA
    in_hbm = pl.BlockSpec(memory_space=pl.ANY)
    in_vmem = pl.BlockSpec(memory_space=pltpu.VMEM)
    sems = {
        "stage": dma((2,)),
        "local": dma((2,)),
        "tok_s": dma((p.n_ra,)),
        "tok_r": dma((p.n_ra,)),
        "toke_s": dma((p.n_ra,)),
        "toke_r": dma((p.n_ra,)),
        "w": dma((n_k, p.n_ra)),
        "z": dma((n_k, p.n_z)),
        "y": dma((n_k, p.n_z, p.n_y)),
        "g0_s": dma((p.n_steps,)),
        "g0_r": dma((p.n_steps,)),
        "g_s": dma((p.n_steps, p.n_chunks)),
        "g_r": dma((p.n_steps, p.n_chunks)),
        "r_s": dma((layers, p.n_steps, p.n_chunks)),
        "r_r": dma((layers, p.n_steps, p.n_chunks)),
        "h_s": dma((layers, 2)),
        "h_r": dma((layers, 2)),
        "o_s": dma((p.n_chunks, p.q)),
        "o_r": dma((p.n_ra,)),
        "oa_s": dma((p.n_steps - 1, p.groups)),
        "oa_r": dma((p.n_steps - 1, p.groups)),
    }
    names = list(sems)
    n_s = p.n_steps

    def body(*refs):
        head, rest = refs[: 11 + 18], refs[11 + 18 :]
        accs, snds, rcvs = rest[:n_s], rest[n_s : 2 * n_s], rest[2 * n_s : 3 * n_s]
        kernel(p, *head, accs, snds, rcvs, dict(zip(names, rest[3 * n_s :])))

    turned = pl.pallas_call(
        body,
        out_shape=jax.ShapeDtypeStruct((p.length, rows), bf16),
        in_specs=[in_hbm] * 4 + [in_vmem] * 6,
        out_specs=in_hbm,
        scratch_shapes=[
            pltpu.VMEM((n_k, p.features, p.half), bf16),
            pltpu.VMEM((n_k, rows, p.half), bf16),
            pltpu.VMEM((2, rows, columns), f32),
            pltpu.VMEM((layers, p.group_tokens, p.features), bf16),
            pltpu.VMEM((p.edge + p.group_tokens, p.half), f32),
            pltpu.VMEM((p.edge + p.group_tokens, p.half), f32),
            pltpu.VMEM((p.group_tokens, p.half), bf16),
            pltpu.VMEM((p.n_ra, p.own, rows), bf16),
            pltpu.VMEM((p.n_ra, p.extra, rows), bf16),
            pltpu.VMEM((p.extra, p.features), bf16),
            pltpu.VMEM((p.extra, p.half), f32),
            pltpu.VMEM((p.extra, p.half), f32),
            pltpu.VMEM((p.extra, 128), f32),
            pltpu.VMEM((p.group_tokens, 128), f32),
            pltpu.VMEM((layers, 2, p.edge, p.half), f32),
            pltpu.VMEM((layers, 2, p.edge, p.half), f32),
            pltpu.VMEM((p.length, rows), bf16),
            pltpu.VMEM((p.n_chunks, p.q, p.own, rows), bf16),
        ]
        + [pltpu.VMEM((p.slots, size, p.chunk), f32) for size in p.sizes]
        + [pltpu.VMEM((p.n_chunks, size, p.chunk), bf16) for size in p.sizes]
        + [pltpu.VMEM((layers, p.n_chunks, size, p.chunk), bf16) for size in p.sizes]
        + [sems[name] for name in names],
        compiler_params=pltpu.CompilerParams(
            collective_id=0, has_side_effects=True, vmem_limit_bytes=66 * 1000 * 1000
        ),
        name="layers",
    )(
        tokens.T,
        up_weight,
        gate_weight,
        down_weight,
        norm_gain,
        up_scale,
        gate_scale,
        jnp.swapaxes(up_taps, 0, 1),
        jnp.swapaxes(gate_taps, 0, 1),
        down_scale,
    )
    return turned.T


def solution(mesh):
    placed = (
        P("ra", None),
        P(),
        P(None, "ra", "cb"),
        P(None, "ra", "cb"),
        P(None, "cb"),
        P(None, "cb"),
        P(None, None, "cb"),
        P(None, None, "cb"),
        P(None, "ra", "cb"),
        P(),
    )
    return jax.shard_map(
        per_device, mesh=mesh, in_specs=placed, out_specs=P("ra", None), check_vma=False
    )
```

```python
import functools

import jax
import jax.numpy as jnp
from jax import lax
from jax.experimental import pallas as pl
from jax.experimental.pallas import tpu as pltpu
from jax.sharding import PartitionSpec as P

EPS = 1e-06
RESIDUAL = 0.5
MESH = pl.DeviceIdType.MESH


def doublings(low, high):
    bits = []
    while low < high:
        bits.append(low)
        low *= 2
    return bits


def bit_of(value, bit):
    return lax.rem(lax.div(value, bit), 2) if not isinstance(value, int) else (value // bit) % 2


def flip(value, offset):
    for bit in doublings(1, offset + 1):
        if offset & bit:
            value = value + bit - 2 * bit * bit_of(value, bit)
    return value


class Plan:
    def __init__(self, n_ra, n_cb, rows, columns, length, layers, width):
        self.n_ra, self.n_cb, self.rows, self.columns = n_ra, n_cb, rows, columns
        self.length, self.layers, self.width = length, layers, width
        self.n_y = 1 << ((n_ra.bit_length() - 1) // 2)
        self.n_z = n_ra // self.n_y
        self.half = columns // 2
        self.groups = n_ra // 2
        self.group_tokens = length // self.groups
        self.cb_bits = doublings(1, n_cb)
        self.n_steps = len(self.cb_bits) + 1
        self.sizes = [self.group_tokens >> (s + 1) for s in range(self.n_steps)]
        self.own = self.sizes[-1]
        self.q = 1
        while rows * self.q < 256 and self.q < self.n_y:
            self.q *= 2
        self.chunk = rows * self.q
        self.n_chunks = n_ra // self.q
        self.features = n_ra * rows
        cy = self.n_y // self.q
        self.cy = cy
        self.order_bits = [cy] + doublings(1, cy) + doublings(2 * cy, self.n_z * cy)
        self.edge = 8
        self.extra = 16
        self.slots = 3


def kernel(
    p,
    tin,
    up_w,
    gate_w,
    down_w,
    gain,
    up_scale,
    gate_scale,
    up_taps,
    gate_taps,
    down_scale,
    out,
    w,
    give,
    stage,
    st,
    up,
    gate,
    hid,
    tok,
    tok_e,
    st_e,
    up_e,
    gate_e,
    sq_e,
    sq,
    tail,
    halo,
    obuf,
    ost,
    accs,
    snds,
    rcvs,
    sem,
):
    r, j = lax.axis_index("ra"), lax.axis_index("cb")
    z, y = lax.div(r, p.n_y), lax.rem(r, p.n_y)
    m = lax.rem(z, 2)
    mine = [bit_of(j, bit) for bit in p.cb_bits] + [m]
    n_k = 3 * p.layers

    def group_of(dev):
        return lax.div(lax.div(dev, p.n_y), 2) * p.n_y + lax.rem(dev, p.n_y)

    def sub_row(bits, count):
        start = 0
        for s in range(count):
            start = start + bits[s] * p.sizes[s]
        return start

    def first_token(dev):
        bits = mine[:-1] + [lax.rem(lax.div(dev, p.n_y), 2)]
        return group_of(dev) * p.group_tokens + sub_row(bits, p.n_steps)

    def partner(s):
        if s < p.n_steps - 1:
            return r, flip(j, p.cb_bits[s])
        return flip(r, p.n_y), j

    def copy(src, dst, ssem, rsem, dev):
        return pltpu.make_async_remote_copy(
            src_ref=src,
            dst_ref=dst,
            send_sem=ssem,
            recv_sem=rsem,
            device_id=dev,
            device_id_type=MESH,
        )

    def at_rows(start, size):
        return pl.ds(pl.multiple_of(start, size), size)

    own_row = sub_row(mine, p.n_steps)
    own_rows = at_rows(own_row, p.own)
    my_slab = at_rows(r * p.rows, p.rows)

    barrier = pltpu.get_barrier_semaphore()
    for off in range(1, p.n_ra):
        pl.semaphore_signal(barrier, inc=1, device_id=(flip(r, off), j), device_id_type=MESH)
    for bit in p.cb_bits:
        pl.semaphore_signal(barrier, inc=1, device_id=(r, flip(j, bit)), device_id_type=MESH)

    def load(k):
        layer, kind = k // 3, k % 3
        source = (up_w, gate_w, down_w)[kind]
        return pltpu.make_async_copy(source.at[layer], stage.at[k % 2], sem["stage"].at[k % 2])

    load(0).start()
    load(1).start()
    own_tokens = pltpu.make_async_copy(
        tin.at[at_rows(first_token(r), p.own)], tok.at[r], sem["local"].at[0]
    )
    own_tokens.start()
    group = group_of(r)

    def extra_rows(dev):
        return at_rows(group_of(dev) * p.group_tokens - p.extra, p.extra)

    own_extra = pltpu.make_async_copy(tin.at[extra_rows(r)], tok_e.at[r], sem["local"].at[1])

    @pl.when(group > 0)
    def _():
        own_extra.start()

    def token_send(off):
        dev = flip(r, off)
        return copy(
            tin.at[at_rows(first_token(dev), p.own)],
            tok.at[r],
            sem["tok_s"].at[off],
            sem["tok_r"].at[r],
            (dev, j),
        )


    def extra_send(off):
        dev = flip(r, off)
        return copy(
            tin.at[extra_rows(dev)],
            tok_e.at[r],
            sem["toke_s"].at[off],
            sem["toke_r"].at[r],
            (dev, j),
        )

    def slab(k, dev):
        return w.at[k, at_rows(dev * p.rows, p.rows)]

    def z_send(k, dz):
        source = give.at[k] if dz % 2 else slab(k, r)
        return copy(
            source, slab(k, r), sem["z"].at[k, dz], sem["w"].at[k, r], (flip(z, dz) * p.n_y + y, j)
        )

    def y_send(k, dz, dy):
        dev = flip(z, dz) * p.n_y + y
        return copy(
            slab(k, dev),
            slab(k, dev),
            sem["y"].at[k, dz, dy],
            sem["w"].at[k, dev],
            (z * p.n_y + flip(y, dy), j),
        )

    def slab_wait(k, dev):
        copy(slab(k, dev), slab(k, dev), sem["z"].at[k, 0], sem["w"].at[k, dev], (r, j)).wait_recv()

    def forward(k, dz):
        if dz:
            slab_wait(k, flip(z, dz) * p.n_y + y)
        for dy in range(1, p.n_y):
            y_send(k, dz, dy).start()

    def convert(k):
        load(k).wait()
        tile = min(64, p.rows)

        @pl.loop(0, p.rows // tile)
        def _(t):
            rows = at_rows(t * tile, tile)
            keep = stage[k % 2, rows, pl.ds(pl.multiple_of(m * p.half, 128), p.half)]
            rest = stage[k % 2, rows, pl.ds(pl.multiple_of((1 - m) * p.half, 128), p.half)]
            w[k, at_rows(r * p.rows + t * tile, tile), :] = keep.astype(jnp.bfloat16)
            give[k, rows, :] = rest.astype(jnp.bfloat16)

        if k + 2 < n_k:
            load(k + 2).start()

    far = list(range(2, p.n_z))

    def is_inner(plane):
        return jnp.logical_and(plane > 0, plane < p.n_z - 1)

    def far_send(k):
        if k >= 3:
            for dz in far:
                z_send(k, dz).start()
            return
        for wanted in (True, False):
            for dz in far:

                @pl.when(is_inner(flip(z, dz)) == wanted)
                def _():
                    z_send(k, dz).start()

    inner = is_inner(z)

    def block_rows(a):
        count = p.n_steps - a
        size = p.own << a
        return sub_row(mine, count), size

    def gather_copy(layer, a, lanes, ssem, rsem):
        start, size = block_rows(a)
        ref = st.at[layer, at_rows(start, size), lanes]
        return copy(ref, ref, ssem, rsem, partner(p.n_steps - 1 - a))

    def gather_wait(layer, a, lanes, ssem, rsem):
        start, size = block_rows(a)
        s = p.n_steps - 1 - a
        ref = st.at[layer, at_rows(start + (1 - 2 * mine[s]) * size, size), lanes]
        copy(ref, ref, ssem, rsem, (r, j)).wait_recv()

    everything = pl.ds(0, p.features)

    def gather0(a):
        return gather_copy(0, a, everything, sem["g0_s"].at[a], sem["g0_r"].at[a])

    def gather0_wait(a):
        gather_wait(0, a, everything, sem["g0_s"].at[a], sem["g0_r"].at[a])

    convert(0)
    convert(1)
    with jax.named_scope("barrier"):
        pl.semaphore_wait(barrier, p.n_ra - 1 + len(p.cb_bits))
    for off in range(1, p.n_ra):
        token_send(off).start()

        @pl.when(group_of(flip(r, off)) > 0)
        def _():
            extra_send(off).start()

    forward(0, 0)
    forward(1, 0)
    convert(2)
    with jax.named_scope("tokens"):
        own_tokens.wait()
        for src in range(p.n_ra):
            lanes = slice(src * p.rows, (src + 1) * p.rows)

            @pl.when(r != src)
            def _():
                copy(
                    tok.at[src], tok.at[src], sem["tok_s"].at[0], sem["tok_r"].at[src], (r, j)
                ).wait_recv()

            st[0, own_rows, lanes] = tok[src]

    convert(3)
    gather0(0).start()
    z_send(0, 1).start()
    z_send(1, 1).start()

    @pl.when(group > 0)
    def _():
        own_extra.wait()
        for src in range(p.n_ra):

            @pl.when(r != src)
            def _():
                copy(
                    tok_e.at[src], tok_e.at[src], sem["toke_s"].at[0], sem["toke_r"].at[src], (r, j)
                ).wait_recv()

            st_e[:, src * p.rows : (src + 1) * p.rows] = tok_e[src]
        values = st_e[...].astype(jnp.float32)
        total = None
        for c in range(p.features // 128):
            part = values[:, c * 128 : (c + 1) * 128]
            total = part * part if total is None else total + part * part
        sq_e[...] = total

    far_send(0)
    forward(2, 0)
    convert(4)
    forward(3, 0)
    convert(5)
    for a in range(p.n_steps):
        with jax.named_scope(f"gather0#a={a}"):
            gather0_wait(a)
        if a + 1 < p.n_steps:
            gather0(a + 1).start()
        if a == 0:
            far_send(1)
            z_send(2, 1).start()
            z_send(3, 1).start()
        if a == 1:
            far_send(2)
            z_send(4, 1).start()
            z_send(5, 1).start()
        if a < 2:
            with jax.named_scope(f"near#k={a}"):
                forward(a, 1)
        if a == 1:
            for dz in far:
                forward(0, dz)

    def chunk_of(i):
        base = (z - m) * p.cy + lax.div(y, p.q)
        total = 0
        shift = 1
        for bit in p.order_bits:
            total = total + lax.rem(lax.div(base, bit) + lax.div(i, shift), 2) * bit
            shift *= 2
        return total

    def chunk_lanes(f):
        return pl.ds(pl.multiple_of(f * p.chunk, p.chunk), p.chunk)

    def chunk_wait(k, f):
        for t in range(p.q):
            dev = f * p.q + t

            @pl.when(lax.rem(dev, p.n_y) != y)
            def _():
                slab_wait(k, dev)

    tile = min(256, p.group_tokens)
    fine = 64

    def squares(layer, lanes, first):
        @pl.loop(0, p.group_tokens // fine)
        def _(t):
            rows = at_rows(t * fine, fine)
            values = st[layer, rows, lanes].astype(jnp.float32)
            total = None
            for c in range(p.chunk // 128):
                part = values[:, c * 128 : (c + 1) * 128]
                total = part * part if total is None else total + part * part
            if first is None:
                sq[rows, :] = sq[rows, :] + total
            else:

                @pl.when(first)
                def _():
                    sq[rows, :] = total

                @pl.when(jnp.logical_not(first))
                def _():
                    sq[rows, :] = sq[rows, :] + total

    @pl.loop(0, p.n_chunks)
    def _(i):
        squares(0, chunk_lanes(i), i == 0)

    def product_chunk(layer, k, dst, i, first):
        f = chunk_of(i)
        chunk_wait(k, f)
        lanes = chunk_lanes(f)
        weights = w.at[k, at_rows(f * p.chunk, p.chunk)]

        @pl.loop(0, p.group_tokens // tile)
        def _(t):
            rows = at_rows(t * tile, tile)
            scaled = st[layer, rows, lanes].astype(jnp.float32) * gain[layer : layer + 1, lanes]
            term = jnp.dot(
                scaled.astype(jnp.bfloat16), weights[...], preferred_element_type=jnp.float32
            )
            to = pl.ds(pl.multiple_of(p.edge + t * tile, 8), tile)
            dst[to, :] = term if first else dst[to, :] + term

        if layer == 0:

            @pl.when(group > 0)
            def _():
                scaled = st_e[:, lanes].astype(jnp.float32) * gain[layer : layer + 1, lanes]
                term = jnp.dot(
                    scaled.astype(jnp.bfloat16), weights[...], preferred_element_type=jnp.float32
                )
                to = (up_e, gate_e)[k % 3]
                to[...] = term if first else to[...] + term

    def product(layer, k, dst, start, stop):
        if start == 0:
            product_chunk(layer, k, dst, 0, True)

        @pl.loop(max(start, 1), stop)
        def _(i):
            product_chunk(layer, k, dst, i, False)

    def product_stage(layer, k, dst, i):
        @pl.when(i == 0)
        def _():
            product_chunk(layer, k, dst, i, True)

        @pl.when(i > 0)
        def _():
            product_chunk(layer, k, dst, i, False)

    own_half = pl.ds(pl.multiple_of(m * p.half, 128), p.half)
    following = group + 1
    following_dev = (lax.div(following, p.n_y) * 2 + m) * p.n_y + lax.rem(following, p.n_y)

    def halo_copy(layer, which):
        return copy(
            tail.at[layer, which],
            halo.at[layer, which],
            sem["h_s"].at[layer, which],
            sem["h_r"].at[layer, which],
            (following_dev, j),
        )

    def inverse_of(squares_sum):
        total = jnp.sum(squares_sum, axis=1, keepdims=True)
        return lax.rsqrt(total * (1.0 / p.features) + EPS)

    def convolve(layer, between):
        if layer:
            inverse = inverse_of(sq[p.group_tokens - p.edge : p.group_tokens, :])
            ends = slice(p.group_tokens, p.group_tokens + p.edge)
            tail[layer, 0] = up[ends, :] * inverse
            tail[layer, 1] = gate[ends, :] * inverse

            @pl.when(following < p.groups)
            def _():
                halo_copy(layer, 0).start()
                halo_copy(layer, 1).start()

        taps_u = up_taps[:, layer, own_half] * up_scale[layer : layer + 1, own_half]
        taps_g = gate_taps[:, layer, own_half] * gate_scale[layer : layer + 1, own_half]
        low = p.edge + 1 - p.width

        def taps_over(values, taps):
            total = taps[0:1] * values[low : low + fine]
            for c in range(1, p.width):
                total = total + taps[c : c + 1] * values[low + c : low + c + fine]
            return total

        def finish_tile(up_values, gate_values, t):
            conv_gate = taps_over(gate_values, taps_g)
            conv_up = taps_over(up_values, taps_u)
            value = conv_gate / (1.0 + jnp.exp(-conv_gate)) * conv_up
            hid[at_rows(t * fine, fine), :] = value.astype(jnp.bfloat16)

        tiles = p.group_tokens // fine

        @pl.loop(0, tiles - 1)
        def _(step):
            t = tiles - 1 - step
            before = pl.ds(pl.multiple_of(t * fine - p.edge, 8), fine + p.edge)
            inverse = inverse_of(sq[before, :])
            rows = pl.ds(pl.multiple_of(t * fine, 8), fine + p.edge)
            finish_tile(up[rows, :] * inverse, gate[rows, :] * inverse, t)


        if layer:
            between()

        @pl.when(group > 0)
        def _():
            if layer:
                for which, dst in ((0, up), (1, gate)):
                    copy(
                        halo.at[layer, which],
                        halo.at[layer, which],
                        sem["h_s"].at[layer, which],
                        sem["h_r"].at[layer, which],
                        (r, j),
                    ).wait_recv()
                    dst[0 : p.edge, :] = halo[layer, which]
            else:
                inverse = inverse_of(sq_e[...])[p.extra - p.edge :]
                up[0 : p.edge, :] = up_e[p.extra - p.edge :, :] * inverse
                gate[0 : p.edge, :] = gate_e[p.extra - p.edge :, :] * inverse

        @pl.when(group == 0)
        def _():
            up[0 : p.edge, :] = jnp.zeros((p.edge, p.half), jnp.float32)
            gate[0 : p.edge, :] = jnp.zeros((p.edge, p.half), jnp.float32)

        inverse = inverse_of(sq[0:fine, :])
        first = slice(p.edge, p.edge + fine)
        finish_tile(
            jnp.concatenate([up[0 : p.edge, :], up[first, :] * inverse], axis=0),
            jnp.concatenate([gate[0 : p.edge, :], gate[first, :] * inverse], axis=0),
            0,
        )

    def reduce_copy(layer, s, i):
        return copy(
            snds[s].at[i],
            rcvs[s].at[layer, i],
            sem["r_s"].at[layer, s, i],
            sem["r_r"].at[layer, s, i],
            partner(s),
        )

    def reduce_wait(layer, s, i):
        ref = rcvs[s].at[layer, i]
        copy(ref, ref, sem["r_s"].at[layer, s, i], sem["r_r"].at[layer, s, i], (r, j)).wait_recv()

    def down_stage(layer, i):
        k = 3 * layer + 2
        f = chunk_of(i)
        chunk_wait(k, f)
        weights = w.at[k, at_rows(f * p.chunk, p.chunk)]
        size = p.sizes[0]
        step = min(tile, size)

        def term(start):
            return lax.dot_general(
                hid[pl.ds(pl.multiple_of(start, step), step), :],
                weights[...],
                (((1,), (1,)), ((), ())),
                preferred_element_type=jnp.float32,
            )

        @pl.loop(0, size // step)
        def _(t):
            rows = at_rows(t * step, step)
            snds[0][i, rows, :] = term((1 - mine[0]) * size + t * step).astype(jnp.bfloat16)

        @pl.loop(0, size // step)
        def _(t):
            accs[0][lax.rem(i, p.slots), at_rows(t * step, step), :] = term(mine[0] * size + t * step)

        reduce_copy(layer, 0, i).start()

    def reduce_stage(layer, s, i):
        reduce_wait(layer, s - 1, i)
        size = p.sizes[s]
        slot = lax.rem(i, p.slots)
        give_rows = at_rows((1 - mine[s]) * size, size)
        keep_rows = at_rows(mine[s] * size, size)
        arrived = rcvs[s - 1][layer, i, give_rows, :].astype(jnp.float32)
        snds[s][i] = (accs[s - 1][slot, give_rows, :] + arrived).astype(jnp.bfloat16)
        arrived = rcvs[s - 1][layer, i, keep_rows, :].astype(jnp.float32)
        accs[s][slot] = accs[s - 1][slot, keep_rows, :] + arrived
        reduce_copy(layer, s, i).start()

    def gather1(a, f):
        return gather_copy(1, a, chunk_lanes(f), sem["g_s"].at[a, f], sem["g_r"].at[a, f])

    def gather1_wait(a, f):
        gather_wait(1, a, chunk_lanes(f), sem["g_s"].at[a, f], sem["g_r"].at[a, f])

    def out_copy(f, t):
        return copy(
            ost.at[f, t],
            obuf.at[at_rows(first_token(r), p.own)],
            sem["o_s"].at[f, t],
            sem["o_r"].at[r],
            (f * p.q + t, j),
        )

    def last_stage(layer, i):
        f = chunk_of(i)
        s = p.n_steps - 1
        reduce_wait(layer, s, i)
        lanes = chunk_lanes(f)
        total = accs[s][lax.rem(i, p.slots)] + rcvs[s][layer, i].astype(jnp.float32)
        before = st[layer, own_rows, lanes].astype(jnp.float32)
        value = total * down_scale[layer : layer + 1, lanes] + RESIDUAL * before
        value = value.astype(jnp.bfloat16)
        if layer + 1 < p.layers:
            st[layer + 1, own_rows, lanes] = value
            gather1(0, f).start()
        else:
            for t in range(p.q):
                ost[f, t] = value[:, t * p.rows : (t + 1) * p.rows]
                dev = f * p.q + t

                @pl.when(dev == r)
                def _():
                    obuf[at_rows(first_token(r), p.own), :] = ost[f, t]

                @pl.when(dev != r)
                def _():
                    out_copy(f, t).start()

    def gather_stage(a, i):
        f = chunk_of(i)
        gather1_wait(a, f)
        if a + 1 < p.n_steps:
            gather1(a + 1, f).start()
        else:
            squares(1, chunk_lanes(f), i == 0)
            product_stage(1, 3, up, i)

    def pipeline(stages, tasks):
        count = p.n_chunks + stages[-1][0]

        @pl.loop(0, count)
        def _(it):
            for back, (lag, stage) in reversed(list(enumerate(stages))):
                i = it - lag

                @pl.when(jnp.logical_and(i >= 0, i < p.n_chunks))
                def _():
                    with jax.named_scope(f"stage#b={back}"):
                        stage(i)

            for when, task in tasks:

                @pl.when(it == when)
                def _():
                    task()

    sources = [
        (pz, py)
        for pz in range(0, p.n_z, 2)
        for py in range(p.n_y)
    ]
    n_out = p.n_steps - 1

    def out_rows(index, a, flipped):
        pz, py = sources[index]
        dev = flip(z, pz) * p.n_y + flip(y, py)
        start, size = block_rows(a)
        if flipped:
            start = start + (1 - 2 * mine[p.n_steps - 1 - a]) * size
        return obuf.at[at_rows(group_of(dev) * p.group_tokens + start, size)]

    def out_gather(index, a):
        ref = out_rows(index, a, False)
        return copy(
            ref,
            ref,
            sem["oa_s"].at[a - 1, index],
            sem["oa_r"].at[a - 1, index],
            partner(p.n_steps - 1 - a),
        )

    def out_store(index):
        pz, py = sources[index]
        dev = flip(z, pz) * p.n_y + flip(y, py)
        rows = at_rows(group_of(dev) * p.group_tokens, p.group_tokens)
        return pltpu.make_async_copy(obuf.at[rows], out.at[rows], sem["store"].at[index])

    def out_first(index):
        pz, py = sources[index]
        for low in range(2):
            dev = flip(z - m + low, pz) * p.n_y + flip(y, py)

            @pl.when(dev != r)
            def _():
                with jax.named_scope(f"out0#i={index}"):
                    ref = obuf.at[at_rows(first_token(dev), p.own)]
                    copy(ref, ref, sem["o_s"].at[0, 0], sem["o_r"].at[dev], (r, j)).wait_recv()

        out_gather(index, 1).start()

    def halo_done(layer):
        @pl.when(following < p.groups)
        def _():
            halo_copy(layer, 0).wait_send()
            halo_copy(layer, 1).wait_send()

    def far_forward(k, part=slice(None)):
        with jax.named_scope(f"far#k={k}"):
            for dz in far[part]:
                forward(k, dz)

    def near_forward(k):
        with jax.named_scope(f"near#k={k}"):
            forward(k, 1)

    for layer in range(p.layers):
        last = layer + 1 == p.layers
        k = 3 * layer
        if layer == 0:
            far_send(3)
            with jax.named_scope(f"up#l={layer}"):
                product(layer, k, up, 0, p.n_chunks)
            far_forward(1)
            near_forward(2)
        with jax.named_scope(f"gate#l={layer}"):
            if layer:
                product(layer, k + 1, gate, 0, p.n_chunks - 2)
                far_forward(5, slice(1))
                product(layer, k + 1, gate, p.n_chunks - 2, p.n_chunks)
            else:
                product(layer, k + 1, gate, 0, p.n_chunks)
        with jax.named_scope(f"convolve#l={layer}"):
            convolve(layer, lambda: far_forward(5, slice(1, None)))
        if layer == 0:

            @pl.when(inner)
            def _():
                far_send(4)
                far_send(5)

        stages = [(0, functools.partial(down_stage, layer))]
        lag = 1
        for step in range(1, p.n_steps):
            stages.append((lag, functools.partial(reduce_stage, layer, step)))
            lag += 2
        stages.append((lag, functools.partial(last_stage, layer)))
        tasks = []
        if not last:
            for step in range(p.n_steps):
                lag += 2 if step + 1 < p.n_steps else 1
                stages.append((lag, functools.partial(gather_stage, step)))

            def outer_send(k):
                @pl.when(jnp.logical_not(inner))
                def _():
                    far_send(k)

            tasks = [
                (1, lambda: far_forward(2)),
                (2, lambda: near_forward(3)),
                (2, lambda: forward(4, 0)),
                (3, lambda: near_forward(4)),
                (3, lambda: forward(5, 0)),
                (5, lambda: near_forward(5)),
                (8, lambda: outer_send(4)),
                (9, lambda: far_forward(3, slice(1))),
                (10, lambda: far_forward(3, slice(1, None))),
                (12, lambda: outer_send(5)),
                (13, lambda: far_forward(4, slice(1))),
                (15, lambda: far_forward(4, slice(1, None))),
            ]
        else:
            count = p.n_chunks + lag
            early = [index for index in range(p.groups) if p.q == 1 and 2 * index + 4 + lag < count]
            tasks += [
                (2 * index + 4 + lag, functools.partial(out_first, index)) for index in early
            ]
        with jax.named_scope(f"down#l={layer}"):
            pipeline(stages, tasks)

        @pl.loop(0, p.n_chunks)
        def _(i):
            for s in range(p.n_steps):
                reduce_copy(layer, s, i).wait_send()

        if last:
            halo_done(layer)

    for index in range(len(sources)):
        if index not in early:
            out_first(index)
    for a in range(1, p.n_steps):
        for index in range(len(sources)):
            ref = out_rows(index, a, True)
            with jax.named_scope(f"out{a}#i={index}"):
                copy(
                    ref, ref, sem["oa_s"].at[a - 1, index], sem["oa_r"].at[a - 1, index], (r, j)
                ).wait_recv()
            if a + 1 < p.n_steps:
                out_gather(index, a + 1).start()
            else:
                out_store(index).start()

    finish = jax.named_scope("finish")
    finish.__enter__()
    for off in range(1, p.n_ra):
        token_send(off).wait_send()

        @pl.when(group_of(flip(r, off)) > 0)
        def _():
            extra_send(off).wait_send()

    for k in range(n_k):
        for dz in range(1, p.n_z):
            z_send(k, dz).wait_send()
        for dz in range(p.n_z):
            for dy in range(1, p.n_y):
                y_send(k, dz, dy).wait_send()
    for a in range(p.n_steps):
        gather0(a).wait_send()

    @pl.loop(0, p.n_chunks)
    def _(f):
        for a in range(p.n_steps):
            gather1(a, f).wait_send()
        for t in range(p.q):

            @pl.when(f * p.q + t != r)
            def _():
                out_copy(f, t).wait_send()

    for a in range(1, p.n_steps):
        for index in range(len(sources)):
            out_gather(index, a).wait_send()
    for index in range(len(sources)):
        out_store(index).wait()
    finish.__exit__(None, None, None)


def per_device(
    tokens,
    norm_gain,
    up_weight,
    gate_weight,
    up_scale,
    gate_scale,
    up_taps,
    gate_taps,
    down_weight,
    down_scale,
):
    layers, rows, columns = up_weight.shape
    p = Plan(
        lax.axis_size("ra"),
        lax.axis_size("cb"),
        rows,
        columns,
        tokens.shape[1],
        layers,
        up_taps.shape[1],
    )
    n_k = 3 * layers
    bf16, f32 = jnp.bfloat16, jnp.float32
    dma = pltpu.SemaphoreType.DMA
    in_hbm = pl.BlockSpec(memory_space=pl.ANY)
    in_vmem = pl.BlockSpec(memory_space=pltpu.VMEM)
    sems = {
        "stage": dma((2,)),
        "local": dma((2,)),
        "store": dma((p.groups,)),
        "tok_s": dma((p.n_ra,)),
        "tok_r": dma((p.n_ra,)),
        "toke_s": dma((p.n_ra,)),
        "toke_r": dma((p.n_ra,)),
        "w": dma((n_k, p.n_ra)),
        "z": dma((n_k, p.n_z)),
        "y": dma((n_k, p.n_z, p.n_y)),
        "g0_s": dma((p.n_steps,)),
        "g0_r": dma((p.n_steps,)),
        "g_s": dma((p.n_steps, p.n_chunks)),
        "g_r": dma((p.n_steps, p.n_chunks)),
        "r_s": dma((layers, p.n_steps, p.n_chunks)),
        "r_r": dma((layers, p.n_steps, p.n_chunks)),
        "h_s": dma((layers, 2)),
        "h_r": dma((layers, 2)),
        "o_s": dma((p.n_chunks, p.q)),
        "o_r": dma((p.n_ra,)),
        "oa_s": dma((p.n_steps - 1, p.groups)),
        "oa_r": dma((p.n_steps - 1, p.groups)),
    }
    names = list(sems)
    n_s = p.n_steps

    def body(*refs):
        head, rest = refs[: 11 + 18], refs[11 + 18 :]
        accs, snds, rcvs = rest[:n_s], rest[n_s : 2 * n_s], rest[2 * n_s : 3 * n_s]
        kernel(p, *head, accs, snds, rcvs, dict(zip(names, rest[3 * n_s :])))

    turned = pl.pallas_call(
        body,
        out_shape=jax.ShapeDtypeStruct((p.length, rows), bf16),
        in_specs=[in_hbm] * 4 + [in_vmem] * 6,
        out_specs=in_hbm,
        scratch_shapes=[
            pltpu.VMEM((n_k, p.features, p.half), bf16),
            pltpu.VMEM((n_k, rows, p.half), bf16),
            pltpu.VMEM((2, rows, columns), f32),
            pltpu.VMEM((layers, p.group_tokens, p.features), bf16),
            pltpu.VMEM((p.edge + p.group_tokens, p.half), f32),
            pltpu.VMEM((p.edge + p.group_tokens, p.half), f32),
            pltpu.VMEM((p.group_tokens, p.half), bf16),
            pltpu.VMEM((p.n_ra, p.own, rows), bf16),
            pltpu.VMEM((p.n_ra, p.extra, rows), bf16),
            pltpu.VMEM((p.extra, p.features), bf16),
            pltpu.VMEM((p.extra, p.half), f32),
            pltpu.VMEM((p.extra, p.half), f32),
            pltpu.VMEM((p.extra, 128), f32),
            pltpu.VMEM((p.group_tokens, 128), f32),
            pltpu.VMEM((layers, 2, p.edge, p.half), f32),
            pltpu.VMEM((layers, 2, p.edge, p.half), f32),
            pltpu.VMEM((p.length, rows), bf16),
            pltpu.VMEM((p.n_chunks, p.q, p.own, rows), bf16),
        ]
        + [pltpu.VMEM((p.slots, size, p.chunk), f32) for size in p.sizes]
        + [pltpu.VMEM((p.n_chunks, size, p.chunk), bf16) for size in p.sizes]
        + [pltpu.VMEM((layers, p.n_chunks, size, p.chunk), bf16) for size in p.sizes]
        + [sems[name] for name in names],
        compiler_params=pltpu.CompilerParams(
            collective_id=0, has_side_effects=True, vmem_limit_bytes=66 * 1000 * 1000
        ),
        name="layers",
    )(
        tokens.T,
        up_weight,
        gate_weight,
        down_weight,
        norm_gain,
        up_scale,
        gate_scale,
        jnp.swapaxes(up_taps, 0, 1),
        jnp.swapaxes(gate_taps, 0, 1),
        down_scale,
    )
    return turned.T


def solution(mesh):
    placed = (
        P("ra", None),
        P(),
        P(None, "ra", "cb"),
        P(None, "ra", "cb"),
        P(None, "cb"),
        P(None, "cb"),
        P(None, None, "cb"),
        P(None, None, "cb"),
        P(None, "ra", "cb"),
        P(),
    )
    return jax.shard_map(
        per_device, mesh=mesh, in_specs=placed, out_specs=P("ra", None), check_vma=False
    )
```
